256 devices in a mesh: ra: 16 (over y, x), cb: 16 (over z, core).
Axes of the slice: x: 4, y: 4, z: 8, core: 2. Of those that a mesh axis runs over, the one named last changes fastest.
Arguments:
- tokens: bfloat16 [512, 4096], P(None, 'ra'), may hold values from -40 to 40, as said below
- norm_gain: float32 [2, 4096], P(None, 'ra'), may hold values from 0.1 to 1.9
- gate_weight: bfloat16 [2, 4096, 11264], P(None, 'ra', 'cb'), may hold values from -0.09375 to 0.09375
- up_weight: bfloat16 [2, 4096, 11264], P(None, 'ra', 'cb'), may hold values from -0.09375 to 0.09375
- down_weight: bfloat16 [2, 11264, 4096], P(None, 'cb', 'ra'), may hold values from -0.0546875 to 0.0546875
Outputs:
- result: bfloat16 [512, 4096], P(None, 'ra')
The draws below stay inside these ranges and needn't reach their ends.
Inputs may be any that keep to these rules, and one draw needn't show every extreme that they name: `tokens`: features come in blocks of 32 with scales that differ from block to block by up to a factor of 16.
All inputs are finite; a program needn't handle non-finite values.
Results may differ from the reference program's by a relative error of at most 0.0075.
Values may be sent and summed in bfloat16 or wider, within the bound.
A program may use at most 64 MiB of HBM per device.

```python
import jax
import jax.numpy as jnp
from jax import lax

D = 4096
FF = 11264
TOKENS = 512
LAYERS = 2


def draw_tokens(key, part):
    first, second, third = jax.random.split(key, 3)
    base = jax.random.normal(first, (TOKENS, D), jnp.float32)
    blocks = jax.random.uniform(second, (D // 32,), jnp.float32, -1.0, 1.0)
    factor = jnp.repeat(4.0 ** blocks, 32)
    values = base * factor
    return jnp.clip(values, -40.0, 40.0).astype(jnp.bfloat16)


def levels(rng, extent, cuts, low, largest):
    def one(dim, shards_of):
        heights = jax.random.uniform(jax.random.fold_in(jax.random.fold_in(rng, 6), dim), (shards_of,), jnp.float32, low / len(cuts), largest / len(cuts))
        return jnp.repeat(jnp.exp(heights), extent[dim] // shards_of).reshape((-1,) + (1,) * (len(extent) - dim - 1))

    level = one(*cuts[0])
    for cut in cuts[1:]:
        level = level * one(*cut)
    return level


def normal_values(key, shape, deviation, limit, cuts=(), kind=jnp.bfloat16):
    factor_of = levels(key, shape, cuts, -0.22, 0.18) if cuts else 1.0
    values = jax.random.normal(key, shape, jnp.float32) * deviation * factor_of
    return jnp.minimum(jnp.maximum(values, -limit), limit).astype(kind)


def setup_inputs(seed: int = 0) -> dict:
    seeds = jax.random.split(jax.random.key(seed), 6)
    tokens = draw_tokens(jax.random.fold_in(seeds[5], 71), 0)
    norm_gain = jnp.clip(1.0 + 0.18 * jax.random.normal(seeds[1], (LAYERS, D), jnp.float32), 0.1, 1.9)
    gate_weight = normal_values(seeds[2], (LAYERS, D, FF), D ** -0.5, 0.09375, ((1, 16), (2, 16)))
    up_weight = normal_values(seeds[3], (LAYERS, D, FF), D ** -0.5, 0.09375, ((1, 16), (2, 16)))
    down_weight = normal_values(seeds[4], (LAYERS, FF, D), FF ** -0.5, 0.0546875, ((1, 16), (2, 16)))
    return {"tokens": tokens, "norm_gain": norm_gain, "gate_weight": gate_weight, "up_weight": up_weight, "down_weight": down_weight}


epsilon = 1e-06
keep_share = 0.5

def sublayer(stream, gain, gate_w, up_w, down_w):
    widened = stream.astype(jnp.float32)
    scale = lax.rsqrt(lax.optimization_barrier(jnp.mean(widened * widened, axis=-1, keepdims=True)) + epsilon)
    normed = (widened * gain).astype(jnp.bfloat16)
    gate = jnp.dot(normed, gate_w, preferred_element_type=jnp.float32) * scale
    up_val = jnp.dot(normed, up_w, preferred_element_type=jnp.float32) * scale
    hidden = (jax.nn.silu(gate) * up_val).astype(jnp.bfloat16)
    branch = jnp.dot(hidden, down_w, preferred_element_type=jnp.float32)
    return (keep_share * widened + branch).astype(jnp.bfloat16)

def reference(tokens, norm_gain, gate_weight, up_weight, down_weight):
    stream = tokens
    for layer in range(LAYERS):
        stream = sublayer(stream, norm_gain[layer], gate_weight[layer], up_weight[layer], down_weight[layer])
    return stream
```

```python
import functools

import jax
import jax.numpy as jnp
from jax import lax
from jax.experimental import pallas as pl
from jax.experimental.pallas import tpu as pltpu
from jax.sharding import Mesh
from jax.sharding import PartitionSpec as P

MESH = pl.DeviceIdType.MESH
LAYERS = 2
EPSILON = 1e-06
KEEP = 0.5
F32 = jnp.float32
BF16 = jnp.bfloat16


def far_first(n):
    return sorted(range(1, n), key=lambda d: (-min(d, n - d), d))


def kernel(n, nz, features, tok, gain, wg, wu, wd, out, *scratch):
    (
        stream, gains, graw, uraw, wcat, down,
        send1, recv1, own1, send2, recv2, own2, hid, part, send3, recv3,
        load_sem, peer_sem, s1, r1, s2, r2, s3, r3, s4, r4, s5, r5, s6, r6, s7, r7,
    ) = scratch
    y, x, z, c = (lax.axis_index(a) for a in ("y", "x", "z", "c"))
    half = stream.shape[1] * stream.shape[2]
    group = half // n
    rows = group // n
    zrows = half // nz
    width = wg.shape[2]
    p = c * x + (1 - c) * y
    q = c * y + (1 - c) * x

    def p_peer(d):
        return {"y": lax.rem(y + (1 - c) * d, n), "x": lax.rem(x + c * d, n)}

    def q_peer(d):
        return {"y": lax.rem(y + c * d, n), "x": lax.rem(x + (1 - c) * d, n)}

    def z_peer(d):
        return {"z": lax.rem(z + d, nz)}

    other = {"c": 1 - c}
    pending = []

    def send(src, dst, ss, rs, to):
        copy = pltpu.make_async_remote_copy(src, dst, ss, rs, device_id=to, device_id_type=MESH)
        copy.start()
        pending.append(copy)
        return copy

    barrier = pltpu.get_barrier_semaphore()
    greeted = [p_peer(d) for d in range(1, n)] + [q_peer(d) for d in range(1, n)]
    greeted += [z_peer(d) for d in range(1, nz)] + [other]
    for peer in greeted:
        pl.semaphore_signal(barrier, 1, device_id=peer, device_id_type=MESH)

    loads = [
        pltpu.make_async_copy(wg.at[0], graw.at[0, 0], load_sem.at[0]),
        pltpu.make_async_copy(wu.at[0], uraw.at[0, 0], load_sem.at[1]),
        pltpu.make_async_copy(gain, gains, load_sem.at[2]),
        pltpu.make_async_copy(wg.at[1], graw.at[1, 0], load_sem.at[3]),
        pltpu.make_async_copy(wu.at[1], uraw.at[1, 0], load_sem.at[4]),
        pltpu.make_async_copy(wd.at[0], down.at[0, 0], load_sem.at[5]),
        pltpu.make_async_copy(wd.at[1], down.at[1, 0], load_sem.at[6]),
    ]
    token_loads = [
        pltpu.make_async_copy(tok.at[pl.ds(c * half + k * zrows, zrows)], stream.at[0, k], load_sem.at[7 + k])
        for k in range(nz)
    ]
    for copy in token_loads + loads:
        copy.start()
    for copy in token_loads + loads[:3]:
        copy.wait()

    def join(layer, block):
        wcat[layer, block] = jnp.concatenate([graw[layer, block], uraw[layer, block]], axis=1)

    join(0, 0)
    pl.semaphore_wait(barrier, len(greeted))
    from_peer = []
    for layer in range(LAYERS):
        from_peer.append([
            send(wg.at[layer], graw.at[layer, 1], peer_sem.at[0, layer, 0], peer_sem.at[1, layer, 0], other),
            send(wu.at[layer], uraw.at[layer, 1], peer_sem.at[0, layer, 1], peer_sem.at[1, layer, 1], other),
            send(wd.at[layer], down.at[layer, 1], peer_sem.at[0, layer, 2], peer_sem.at[1, layer, 2], other),
        ])

    first_half = lax.broadcasted_iota(jnp.int32, (1, 128), 1) < 64

    def two_parts(total):
        high = total.astype(BF16).astype(F32)
        return jnp.where(first_half, high, total - high)

    def whole(parts):
        return parts + pltpu.roll(parts, 64, 1)

    for layer in range(LAYERS):
        in_flight = {}
        for block in range(2):
            if block == 1:
                for copy in from_peer[layer][:2]:
                    copy.wait_recv()
                join(layer, 1)
            elif layer > 0:
                for copy in loads[3:5]:
                    copy.wait()
                join(layer, 0)
            for d in far_first(n) + [0]:
                to = lax.rem(p + d, n)
                tokens = stream[layer, pl.ds(to * (nz // n), nz // n)].reshape(group, -1).astype(F32)
                normed = (tokens * gains[pl.ds(layer, 1)]).astype(BF16)
                product = jnp.dot(normed, wcat[layer, block], preferred_element_type=F32)
                if block == 0:
                    squares = jnp.sum(tokens * tokens, axis=1, keepdims=True)
                    squares = jnp.broadcast_to(squares, (group, 128))
                if d == 0:
                    own1[layer, block, :, : 2 * width] = product
                    if block == 0:
                        own1[layer, 0, :, 2 * width :] = jnp.where(first_half, squares, 0.0)
                else:
                    send1[layer, block, d - 1, :, : 2 * width] = product.astype(BF16)
                    if block == 0:
                        send1[layer, 0, d - 1, :, 2 * width :] = two_parts(squares).astype(BF16)
                    span = slice(None) if block == 0 else pl.ds(0, 2 * width)
                    in_flight[block, d] = send(
                        send1.at[layer, block, d - 1, :, span],
                        recv1.at[layer, block, d - 1, :, span],
                        s1.at[layer, block, d - 1],
                        r1.at[layer, block, d - 1],
                        p_peer(d),
                    )
        second = {}
        for block in range(2):
            for d in range(1, n):
                in_flight[block, d].wait_recv()
            w = 2 * width + 128 if block == 0 else 2 * width
            for d in far_first(n) + [0]:
                mine = pl.ds(pl.multiple_of(lax.rem(q + d, n) * rows, rows), rows)
                total = own1[layer, block, mine, :w]
                for e in range(n - 1):
                    total = total + recv1[layer, block, e, mine, :w].astype(F32)
                if block == 0:
                    squares = whole(total[:, 2 * width :])
                    total = total[:, : 2 * width]
                if d == 0:
                    own2[layer, block, :, : 2 * width] = total
                    if block == 0:
                        own2[layer, 0, :, 2 * width :] = jnp.where(first_half, squares, 0.0)
                else:
                    send2[layer, block, d - 1, :, : 2 * width] = total.astype(BF16)
                    if block == 0:
                        send2[layer, 0, d - 1, :, 2 * width :] = two_parts(squares).astype(BF16)
                    span = slice(None) if block == 0 else pl.ds(0, 2 * width)
                    second[block, d] = send(
                        send2.at[layer, block, d - 1, :, span],
                        recv2.at[layer, block, d - 1, :, span],
                        s2.at[layer, block, d - 1],
                        r2.at[layer, block, d - 1],
                        q_peer(d),
                    )
        shares = []
        for block in range(2):
            for d in range(1, n):
                second[block, d].wait_recv()
            w = 2 * width + 128 if block == 0 else 2 * width
            total = own2[layer, block, :, :w]
            for e in range(n - 1):
                total = total + recv2[layer, block, e, :, :w].astype(F32)
            if block == 0:
                squares = whole(total[:, 2 * width :])
                scale = lax.rsqrt(squares[:, :1] / features + EPSILON)
            gate = total[:, :width] * scale
            up = total[:, width : 2 * width] * scale
            shares.append(gate / (1.0 + jnp.exp(-gate)) * up)
        hid[layer, p, q] = jnp.concatenate(shares, axis=1).astype(BF16)
        gathered = [
            send(hid.at[layer, p, q], hid.at[layer, p, q], s3.at[layer, d - 1], r3.at[layer, d - 1], q_peer(d))
            for d in far_first(n)
        ]
        for copy in gathered:
            copy.wait_recv()
        groups = {
            d: send(hid.at[layer, p], hid.at[layer, p], s4.at[layer, d - 1], r4.at[layer, d - 1], p_peer(d))
            for d in far_first(n)
        }
        loads[5 + layer].wait()
        from_peer[layer][2].wait_recv()
        for d in [0] + far_first(n)[::-1]:
            if d:
                groups[d].wait_recv()
            sender = lax.rem(p + n - d, n)
            units = hid[layer, sender].reshape(group, 2 * width)
            weights = down[layer].reshape(2 * width, -1)
            product = jnp.dot(units, weights, preferred_element_type=F32)
            part[layer, pl.ds(sender * (nz // n), nz // n)] = product.reshape(nz // n, zrows, -1)
        down_parts = []
        for d in far_first(nz):
            send3[layer, d - 1] = part[layer, lax.rem(z + d, nz)].astype(BF16)
            down_parts.append(send(
                send3.at[layer, d - 1], recv3.at[layer, d - 1], s5.at[layer, d - 1], r5.at[layer, d - 1], z_peer(d)
            ))
        branch = part[layer, z]
        for copy in down_parts:
            copy.wait_recv()
        for e in range(nz - 1):
            branch = branch + recv3[layer, e].astype(F32)
        new = (KEEP * stream[layer, z].astype(F32) + branch).astype(BF16)
        if layer + 1 < LAYERS:
            stream[layer + 1, z] = new
            rest = [
                send(stream.at[layer + 1, z], stream.at[layer + 1, z], s6.at[d - 1], r6.at[d - 1], z_peer(d))
                for d in far_first(nz)
            ]
            for copy in rest:
                copy.wait_recv()
        else:
            out[c * nz + z] = new
            rest = {
                d: send(out.at[c * nz + z], out.at[c * nz + z], s7.at[0, d - 1], r7.at[0, d - 1], z_peer(d))
                for d in far_first(nz)
            }
            passed = [send(out.at[c * nz + z], out.at[c * nz + z], s7.at[1, nz - 1], r7.at[1, nz - 1], other)]
            for d in far_first(nz)[::-1]:
                rest[d].wait_recv()
                at = c * nz + lax.rem(z + nz - d, nz)
                passed.append(send(out.at[at], out.at[at], s7.at[1, d - 1], r7.at[1, d - 1], other))
            for copy in passed:
                copy.wait_recv()
    for copy in pending:
        copy.wait_send()


def solution(mesh):
    zc = mesh.shape["cb"]
    n, nz = 4, zc // 2
    if mesh.shape["ra"] != n * n:
        n = 2
    torus = Mesh(mesh.devices.reshape(n, n, nz, 2), ("y", "x", "z", "c"))
    ra, cb = ("y", "x"), ("z", "c")

    def body(tokens, norm_gain, gate_weight, up_weight, down_weight):
        count, depth = tokens.shape
        width = gate_weight.shape[2]
        half = count // 2
        group, rows, zrows = half // n, half // (n * n), half // nz
        wide = 2 * width + 128
        dma = pltpu.SemaphoreType.DMA
        scratch = [
            pltpu.VMEM((LAYERS, nz, zrows, depth), BF16),
            pltpu.VMEM((LAYERS, depth), F32),
            pltpu.VMEM((LAYERS, 2, depth, width), BF16),
            pltpu.VMEM((LAYERS, 2, depth, width), BF16),
            pltpu.VMEM((LAYERS, 2, depth, 2 * width), BF16),
            pltpu.VMEM((LAYERS, 2, width, depth), BF16),
            pltpu.VMEM((LAYERS, 2, n - 1, group, wide), BF16),
            pltpu.VMEM((LAYERS, 2, n - 1, group, wide), BF16),
            pltpu.VMEM((LAYERS, 2, group, wide), F32),
            pltpu.VMEM((LAYERS, 2, n - 1, rows, wide), BF16),
            pltpu.VMEM((LAYERS, 2, n - 1, rows, wide), BF16),
            pltpu.VMEM((LAYERS, 2, rows, wide), F32),
            pltpu.VMEM((LAYERS, n, n, rows, 2 * width), BF16),
            pltpu.VMEM((LAYERS, nz, zrows, depth), F32),
            pltpu.VMEM((LAYERS, nz - 1, zrows, depth), BF16),
            pltpu.VMEM((LAYERS, nz - 1, zrows, depth), BF16),
            dma((7 + nz,)),
            dma((2, LAYERS, 3)),
            *[dma((LAYERS, 2, n - 1))] * 4,
            *[dma((LAYERS, n - 1))] * 4,
            *[dma((LAYERS, nz - 1))] * 2,
            *[dma((nz - 1,))] * 2,
            *[dma((2, nz))] * 2,
        ]
        result = pl.pallas_call(
            functools.partial(kernel, n, nz, depth * n * n),
            out_shape=jax.ShapeDtypeStruct((2 * nz, zrows, depth), BF16),
            in_specs=[pl.BlockSpec(memory_space=pl.ANY)] * 5,
            out_specs=pl.BlockSpec(memory_space=pltpu.VMEM),
            scratch_shapes=scratch,
            compiler_params=pltpu.CompilerParams(
                collective_id=0, has_side_effects=True, vmem_limit_bytes=60 * 1024 * 1024
            ),
        )(tokens, norm_gain, gate_weight, up_weight, down_weight)
        return result.reshape(count, depth)

    in_specs = (P(None, ra), P(None, ra), P(None, ra, cb), P(None, ra, cb), P(None, cb, ra))
    return jax.shard_map(body, mesh=torus, in_specs=in_specs, out_specs=P(None, ra), check_vma=False)
```

```python
import functools

import jax
import jax.numpy as jnp
from jax import lax
from jax.experimental import pallas as pl
from jax.experimental.pallas import tpu as pltpu
from jax.sharding import Mesh
from jax.sharding import PartitionSpec as P

MESH = pl.DeviceIdType.MESH
LAYERS = 2
EPSILON = 1e-06
KEEP = 0.5
F32 = jnp.float32
BF16 = jnp.bfloat16
OVER_LAST = (((1,), (1,)), ((), ()))


def far_first(n):
    return sorted(range(1, n), key=lambda d: (-min(d, n - d), d))


def near_first(n):
    return far_first(n)[::-1]


def kernel(n, nz, features, tok, gain, wg, wu, wd, out, *scratch):
    (
        stream, gains, wcat, down, nbuf, squares, send2, recv2, own2, hid, part, send3, recv3,
        load_sem, gs, gr, ws, wr, ds, dr, ts, tr, s2, r2, s3, r3, s4, r4, s5, r5, s6, r6, s7, r7,
    ) = scratch
    y, x, z, c = (lax.axis_index(a) for a in ("y", "x", "z", "c"))
    _, _, _, zrows, depth = stream.shape
    half = nz * zrows
    group = half // n
    slices = nz // n
    pw = down.shape[2]
    wide = wcat.shape[2]
    halves = n // 2
    p = c * x + (1 - c) * y
    q = c * y + (1 - c) * x

    def p_peer(d):
        return {"y": lax.rem(y + (1 - c) * d, n), "x": lax.rem(x + c * d, n)}

    def q_peer(d):
        return {"y": lax.rem(y + c * d, n), "x": lax.rem(x + (1 - c) * d, n)}

    def z_peer(d):
        return {"z": lax.rem(z + d, nz)}

    other = {"c": 1 - c}
    pending = []

    def copy_to(src, dst, ss, rs, to):
        return pltpu.make_async_remote_copy(src, dst, ss, rs, device_id=to, device_id_type=MESH)

    def send(*where):
        copy = copy_to(*where)
        copy.start()
        pending.append(copy)
        return copy

    barrier = pltpu.get_barrier_semaphore()
    greeted = [p_peer(d) for d in range(1, n)] + [q_peer(d) for d in range(1, n)]
    greeted += [{**peer, "c": 1 - c} for peer in greeted]
    greeted += [z_peer(d) for d in range(1, nz)] + [other]
    for peer in greeted:
        pl.semaphore_signal(barrier, 1, device_id=peer, device_id_type=MESH)

    token_loads = [
        pltpu.make_async_copy(tok.at[pl.ds(c * half + k * zrows, zrows)], stream.at[0, 0, k], load_sem.at[k])
        for k in range(nz)
    ]
    token_loads.append(pltpu.make_async_copy(gain, gains.at[0], load_sem.at[nz]))
    down_loads = [
        [
            pltpu.make_async_copy(
                wd.at[layer, pl.ds(h * pw, pw)], down.at[layer, c * halves + h], load_sem.at[nz + 1 + layer * halves + h]
            )
            for h in range(halves)
        ]
        for layer in range(LAYERS)
    ]
    for copy in token_loads + down_loads[0] + down_loads[1]:
        copy.start()
    wcat[:, :, 2 * pw :, :] = jnp.zeros((LAYERS, n, wide - 2 * pw, depth), BF16)
    for copy in token_loads:
        copy.wait()
    pl.semaphore_wait(barrier, len(greeted))

    first = {0: {}}
    for d in far_first(n):
        first[d] = [
            send(gains.at[0], gains.at[d], gs.at[d - 1], gr.at[d - 1], p_peer(d)),
            send(stream.at[0, 0], stream.at[0, d], ts.at[d - 1], tr.at[d - 1], p_peer(d)),
        ]

    def deal_parts(layer, start):
        for t in range(2):
            a = x if t else y
            for h in range(halves):
                owner = c * halves + h
                d = lax.rem(owner - a + n, n)
                to = {"x" if t else "y": owner, "c": t}
                here = jnp.logical_and(c == t, owner == a)
                for k, w in enumerate((wg, wu)):
                    src = w.at[layer, pl.ds(h * pw, pw)]
                    dst = wcat.at[layer, d, pl.ds(k * pw, pw)]
                    sem = ws.at[layer, t, h, k]

                    @pl.when(jnp.logical_and(here, start))
                    def _():
                        pltpu.make_async_copy(src, dst, wr.at[layer, d, k]).start()

                    @pl.when(jnp.logical_not(here))
                    def _():
                        copy = copy_to(src, dst, sem, wr.at[layer, d, k], to)
                        if start:
                            copy.start()
                        else:
                            copy.wait_send()

    def wait_parts(layer):
        for d in range(n):
            for k in range(2):
                dst = wcat.at[layer, d, pl.ds(k * pw, pw)]
                pltpu.make_async_copy(wg.at[layer, pl.ds(0, pw)], dst, wr.at[layer, d, k]).wait()

    deal_parts(0, True)
    from_other = [
        [
            send(
                wd.at[layer, pl.ds(h * pw, pw)], down.at[layer, c * halves + h],
                ds.at[layer, h], dr.at[layer, h], other,
            )
            for h in range(halves)
        ]
        for layer in range(LAYERS)
    ]

    lane = lax.broadcasted_iota(jnp.int32, (1, 128), 1)

    def in_tile(high, low):
        return jnp.where(lane < 64, 0.0, jnp.where(lane < 96, high, low))

    def normalize(layer, at, slots):
        total = 0.0
        for d in range(n):
            tokens = stream[layer, d, at].astype(F32)
            nbuf[layer, at, :, d * depth : (d + 1) * depth] = (tokens * gains[d, layer : layer + 1]).astype(BF16)
            total = total + jnp.sum(tokens * tokens, axis=1, keepdims=True)
        squares[layer, at] = jnp.broadcast_to(total, (zrows, 128))

    arriving = None
    for layer in range(LAYERS):
        if layer == 0:
            for d in near_first(n):
                for copy in first[d]:
                    copy.wait_recv()
            for k in range(nz):
                normalize(layer, k, n)
        else:
            for e in [0] + near_first(nz):
                for d in near_first(n):
                    arriving[e][d].wait_recv()
                normalize(layer, lax.rem(z + nz - e, nz), n)
        wait_parts(layer)
        sums = {}
        for d in far_first(n) + [0]:
            to = pl.ds(lax.rem(q + d, n) * slices, slices)
            product = 0.0
            for e in range(n):
                normed = nbuf[layer, to, :, e * depth : (e + 1) * depth].reshape(group, depth)
                product = product + lax.dot_general(normed, wcat[layer, e], OVER_LAST, preferred_element_type=F32)
            total = squares[layer, to].reshape(group, 128)
            high = total.astype(BF16).astype(F32)
            last = product[:, wide - 128 :]
            if d == 0:
                own2[layer, :, : wide - 128] = product[:, : wide - 128]
                own2[layer, :, wide - 128 :] = last + in_tile(total, 0.0)
            else:
                send2[layer, d - 1, :, : wide - 128] = product[:, : wide - 128].astype(BF16)
                send2[layer, d - 1, :, wide - 128 :] = (last + in_tile(high, total - high)).astype(BF16)
                sums[d] = send(
                    send2.at[layer, d - 1], recv2.at[layer, d - 1], s2.at[layer, d - 1], r2.at[layer, d - 1], q_peer(d)
                )
        total = own2[layer]
        for d in near_first(n):
            sums[d].wait_recv()
            total = total + recv2[layer, d - 1].astype(F32)
        norm = total[:, wide - 64 : wide - 63] + total[:, wide - 32 : wide - 31]
        scale = lax.rsqrt(norm / features + EPSILON)
        gate = total[:, :pw] * scale
        up = total[:, pw : 2 * pw] * scale
        hid[layer, p, q] = (gate / (1.0 + jnp.exp(-gate)) * up).astype(BF16)
        across = {}
        pieces = {0: {}}

        def spread(e):
            at = hid.at[layer, p, lax.rem(q + n - e, n)]
            pieces[e] = {
                d: send(at, at, s4.at[layer, e, d - 1], r4.at[layer, e, d - 1], p_peer(d)) for d in far_first(n)
            }

        for d in far_first(n):
            at = hid.at[layer, p, q]
            across[d] = send(at, at, s3.at[layer, d - 1], r3.at[layer, d - 1], q_peer(d))
        spread(0)
        for d in near_first(n):
            across[d].wait_recv()
            spread(d)
        for copy in down_loads[layer]:
            copy.wait()
        for copy in from_other[layer]:
            copy.wait_recv()
        for e in [0] + near_first(n):
            for d in near_first(n):
                pieces[e][d].wait_recv()
            at = lax.rem(q + n - e, n)
            product = 0.0
            for k in range(n):
                product = product + jnp.dot(hid[layer, k, at], down[layer, k], preferred_element_type=F32)
            part[layer, pl.ds(at * slices, slices)] = product.reshape(slices, zrows, depth)
        down_parts = {}
        for d in far_first(nz):
            send3[layer, d - 1] = part[layer, lax.rem(z + d, nz)].astype(BF16)
            down_parts[d] = send(
                send3.at[layer, d - 1], recv3.at[layer, d - 1], s5.at[layer, d - 1], r5.at[layer, d - 1], z_peer(d)
            )
        if layer + 1 < LAYERS:
            deal_parts(layer + 1, True)
        branch = part[layer, z]
        for d in near_first(nz):
            down_parts[d].wait_recv()
            branch = branch + recv3[layer, d - 1].astype(F32)
        new = (KEEP * stream[layer, 0, z].astype(F32) + branch).astype(BF16)
        if layer + 1 < LAYERS:
            stream[layer + 1, 0, z] = new
            arriving = {}

            def pass_on(e):
                k = lax.rem(z + nz - e, nz)
                arriving[e] = {
                    d: send(
                        stream.at[layer + 1, 0, k], stream.at[layer + 1, d, k], s6.at[e, d], r6.at[e, d], p_peer(d)
                    )
                    for d in far_first(n)
                }

            at = stream.at[layer + 1, 0, z]
            along = {d: send(at, at, s6.at[d, 0], r6.at[d, 0], z_peer(d)) for d in far_first(nz)}
            pass_on(0)
            for e in near_first(nz):
                along[e].wait_recv()
                pass_on(e)
        else:
            mine = out.at[c * nz + z]
            out[c * nz + z] = new
            rest = {d: send(mine, mine, s7.at[0, d - 1], r7.at[0, d - 1], z_peer(d)) for d in far_first(nz)}
            passed = [send(mine, mine, s7.at[1, nz - 1], r7.at[1, nz - 1], other)]
            for d in near_first(nz):
                rest[d].wait_recv()
                at = out.at[c * nz + lax.rem(z + nz - d, nz)]
                passed.append(send(at, at, s7.at[1, d - 1], r7.at[1, d - 1], other))
            for copy in passed:
                copy.wait_recv()
    for copy in pending:
        copy.wait_send()
    for layer in range(LAYERS):
        deal_parts(layer, False)


def solution(mesh):
    nz = mesh.shape["cb"] // 2
    n = 4 if mesh.shape["ra"] == 16 else 2
    torus = Mesh(mesh.devices.reshape(n, n, nz, 2), ("y", "x", "z", "c"))
    ra, cb = ("y", "x"), ("z", "c")

    def body(tokens, norm_gain, gate_weight, up_weight, down_weight):
        count, depth = tokens.shape
        pw = gate_weight.shape[2] * 2 // n
        half = count // 2
        group, zrows = half // n, half // nz
        wide = pl.cdiv(2 * pw + 64, 128) * 128
        dma = pltpu.SemaphoreType.DMA
        scratch = [
            pltpu.VMEM((LAYERS, n, nz, zrows, depth), BF16),
            pltpu.VMEM((n, LAYERS, depth), F32),
            pltpu.VMEM((LAYERS, n, wide, depth), BF16),
            pltpu.VMEM((LAYERS, n, pw, depth), BF16),
            pltpu.VMEM((LAYERS, nz, zrows, n * depth), BF16),
            pltpu.VMEM((LAYERS, nz, zrows, 128), F32),
            pltpu.VMEM((LAYERS, n - 1, group, wide), BF16),
            pltpu.VMEM((LAYERS, n - 1, group, wide), BF16),
            pltpu.VMEM((LAYERS, group, wide), F32),
            pltpu.VMEM((LAYERS, n, n, group, pw), BF16),
            pltpu.VMEM((LAYERS, nz, zrows, depth), F32),
            pltpu.VMEM((LAYERS, nz - 1, zrows, depth), BF16),
            pltpu.VMEM((LAYERS, nz - 1, zrows, depth), BF16),
            dma((nz + 1 + LAYERS * (n // 2),)),
            *[dma((n - 1,))] * 2,
            dma((LAYERS, 2, n // 2, 2)),
            dma((LAYERS, n, 2)),
            *[dma((LAYERS, n // 2))] * 2,
            *[dma((n - 1,))] * 2,
            *[dma((LAYERS, n - 1))] * 4,
            *[dma((LAYERS, n, n - 1))] * 2,
            *[dma((LAYERS, nz - 1))] * 2,
            *[dma((nz, n))] * 2,
            *[dma((2, nz))] * 2,
        ]
        result = pl.pallas_call(
            functools.partial(kernel, n, nz, depth * n * n),
            out_shape=jax.ShapeDtypeStruct((2 * nz, zrows, depth), BF16),
            in_specs=[pl.BlockSpec(memory_space=pl.ANY)] * 5,
            out_specs=pl.BlockSpec(memory_space=pltpu.VMEM),
            scratch_shapes=scratch,
            compiler_params=pltpu.CompilerParams(
                collective_id=0, has_side_effects=True, vmem_limit_bytes=60 * 1024 * 1024
            ),
        )(tokens, norm_gain, jnp.swapaxes(gate_weight, 1, 2), jnp.swapaxes(up_weight, 1, 2), down_weight)
        return result.reshape(count, depth)

    in_specs = (P(None, ra), P(None, ra), P(None, ra, cb), P(None, ra, cb), P(None, cb, ra))
    return jax.shard_map(body, mesh=torus, in_specs=in_specs, out_specs=P(None, ra), check_vma=False)
```

```python
import functools

import jax
import jax.numpy as jnp
from jax import lax
from jax.experimental import pallas as pl
from jax.experimental.pallas import tpu as pltpu
from jax.sharding import Mesh
from jax.sharding import PartitionSpec as P

MESH = pl.DeviceIdType.MESH
LAYERS = 2
EPSILON = 1e-06
KEEP = 0.5
F32 = jnp.float32
BF16 = jnp.bfloat16
OVER_LAST = (((1,), (1,)), ((), ()))


def far_first(n):
    return sorted(range(1, n), key=lambda d: (-min(d, n - d), d))


def near_first(n):
    return far_first(n)[::-1]


def kernel(n, nz, features, early, tok, gain, wg, wu, wd, out, *scratch):
    (
        tokens, stream, gains, w0, down0, w1, down1, nbuf, squares, own1, send1, recv1, own2, send2, recv2, hid0,
        own4, send4, recv4, hid1, part, send3, recv3,
        load_sem, gs, gr, ws, wr, ds, dr, s1, r1, s2, r2, s4, r4, sq, rq, sp, rp, sz, rz, ss, rs, so, ro,
    ) = scratch
    y, x, z, c = (lax.axis_index(a) for a in ("y", "x", "z", "c"))
    _, _, zrows, depth = stream.shape
    half = nz * zrows
    group = half // n
    rows = group // n
    slices = nz // n
    width = wg.shape[1]
    pw = down1.shape[1]
    wide = w1.shape[1]
    halves = n // 2
    cut = first_cut(width)
    p = c * x + (1 - c) * y
    q = c * y + (1 - c) * x

    def p_peer(d):
        return {"y": lax.rem(y + (1 - c) * d, n), "x": lax.rem(x + c * d, n)}

    def q_peer(d):
        return {"y": lax.rem(y + c * d, n), "x": lax.rem(x + (1 - c) * d, n)}

    def z_peer(d):
        return {"z": lax.rem(z + d, nz)}

    other = {"c": 1 - c}
    pending = []

    def copy_to(src, dst, ss, rs, to):
        return pltpu.make_async_remote_copy(src, dst, ss, rs, device_id=to, device_id_type=MESH)

    def send(*where):
        copy = copy_to(*where)
        copy.start()
        pending.append(copy)
        return copy

    barrier = pltpu.get_barrier_semaphore()
    greeted = [p_peer(d) for d in range(1, n)] + [q_peer(d) for d in range(1, n)]
    greeted += [{**peer, "c": 1 - c} for peer in greeted]
    greeted += [z_peer(d) for d in range(1, nz)] + [other]
    for peer in greeted:
        pl.semaphore_signal(barrier, 1, device_id=peer, device_id_type=MESH)

    loads = [
        pltpu.make_async_copy(gain, gains.at[0], load_sem.at[0]),
        pltpu.make_async_copy(tok, tokens, load_sem.at[1]),
        pltpu.make_async_copy(wg.at[0], w0.at[pl.ds(0, width)], load_sem.at[2]),
        pltpu.make_async_copy(wu.at[0], w0.at[pl.ds(width, width)], load_sem.at[3]),
    ]
    down_loads = [[pltpu.make_async_copy(wd.at[0], down0.at[0], load_sem.at[4])], [
        pltpu.make_async_copy(wd.at[1, pl.ds(h * pw, pw)], down1.at[c * halves + h], load_sem.at[5 + h])
        for h in range(halves)
    ]]
    for copy in loads + down_loads[0] + down_loads[1]:
        copy.start()
    w1[:, 2 * pw :, :] = jnp.zeros((n, wide - 2 * pw, depth), BF16)

    lane = lax.broadcasted_iota(jnp.int32, (1, 128), 1)
    edge = wide - 128

    def in_tile(high, low):
        return jnp.where(lane < 64, 0.0, jnp.where(lane < 96, high, low))

    def two_parts(total):
        high = total.astype(BF16).astype(F32)
        return in_tile(high, total - high)

    def all_squares(tile):
        return tile[:, 64:65] + tile[:, 96:97]

    for copy in loads:
        copy.wait()
    for at in range(2):
        mine = tokens[pl.ds((c if at == 0 else 1 - c) * half, half)].astype(F32)
        normed = (mine * gains[0, 0:1]).astype(BF16)
        product = lax.dot_general(normed, w0[...], OVER_LAST, preferred_element_type=F32)
        send1[at, :, :, 128:] = product.astype(BF16).reshape(n, group, 2 * width)
        if at == 0:
            own1[:, :, 128:] = product.reshape(n, group, 2 * width)
            total = jnp.sum(mine * mine, axis=1, keepdims=True)
            own1[:, :, :128] = in_tile(total, 0.0).reshape(n, group, 128)
            send1[0, :, :, :128] = two_parts(total).astype(BF16).reshape(n, group, 128)
    pl.semaphore_wait(barrier, len(greeted))

    spans = [[pl.ds(0, 128 + cut), pl.ds(128 + cut, 2 * width - cut)], [pl.ds(128, cut), pl.ds(128 + cut, 2 * width - cut)]]
    first = {}
    for piece in range(2):
        for d in far_first(n) + [0]:
            for at in range(2):
                if at == 0 and d == 0:
                    continue
                to = lax.rem((p, q)[at] + d, n)
                first[piece, at, d] = send(
                    send1.at[at, to, :, spans[at][piece]],
                    recv1.at[at, d, :, spans[at][piece]],
                    s1.at[piece, at, d],
                    r1.at[piece, at, d],
                    {**(p_peer, q_peer)[at](d), "c": (c, 1 - c)[at]},
                )
    for d in far_first(n):
        send(gains.at[0], gains.at[d], gs.at[d - 1], gr.at[d - 1], p_peer(d))
    from_other = [[send(wd.at[0], down0.at[1], ds.at[0], dr.at[0], other)], [
        send(wd.at[1, pl.ds(h * pw, pw)], down1.at[c * halves + h], ds.at[1 + h], dr.at[1 + h], other)
        for h in range(halves)
    ]]

    def deal_parts(kinds, start):
        for t in range(2):
            a = x if t else y
            for h in range(halves):
                owner = c * halves + h
                d = lax.rem(owner - a + n, n)
                to = {"x" if t else "y": owner, "c": t}
                here = jnp.logical_and(c == t, owner == a)
                for k in kinds:
                    src = (wg, wu)[k].at[1, pl.ds(h * pw, pw)]
                    dst = w1.at[d, pl.ds(k * pw, pw)]
                    sem = ws.at[t, h, k]

                    @pl.when(jnp.logical_and(here, start))
                    def _():
                        pltpu.make_async_copy(src, dst, wr.at[d, k]).start()

                    @pl.when(jnp.logical_not(here))
                    def _():
                        copy = copy_to(src, dst, sem, wr.at[d, k], to)
                        if start:
                            copy.start()
                        else:
                            copy.wait_send()

    second = {}
    bounds = [0, 128 + 2 * cut, 128 + 4 * width]
    for piece in range(2):
        for d in near_first(n) + [0]:
            for at in range(2):
                if at == 1 or d:
                    first[piece, at, d].wait_recv()
        for d in far_first(n) + [0]:
            at = pl.ds(pl.multiple_of(lax.rem(q + d, n) * rows, rows), rows)
            mine = own1[p, at, spans[0][piece]]
            for e in range(1, n):
                mine = mine + recv1[0, e, at, spans[0][piece]].astype(F32)
            theirs = recv1[1, 0, at, spans[1][piece]].astype(F32)
            for e in range(1, n):
                theirs = theirs + recv1[1, e, at, spans[1][piece]].astype(F32)
            total = [mine, theirs]
            if piece == 0:
                norm = all_squares(mine[:, :128])
                tile = two_parts(norm) if d else in_tile(norm, 0.0)
                total = [tile, mine[:, 128:], theirs]
            total = jnp.concatenate(total, axis=1)
            span = pl.ds(bounds[piece], bounds[piece + 1] - bounds[piece])
            if d == 0:
                own2[:, span] = total
            else:
                send2[d - 1, :, span] = total.astype(BF16)
                second[piece, d] = send(
                    send2.at[d - 1, :, span], recv2.at[d - 1, :, span],
                    s2.at[piece, d - 1], r2.at[piece, d - 1], q_peer(d),
                )
    sums = []
    for piece in range(2):
        span = pl.ds(bounds[piece], bounds[piece + 1] - bounds[piece])
        total = own2[:, span]
        for d in near_first(n):
            second[piece, d].wait_recv()
            total = total + recv2[d - 1, :, span].astype(F32)
        sums.append(total)
    scale = lax.rsqrt(all_squares(sums[0][:, :128]) / features + EPSILON)
    rest = 2 * width - cut
    shares = []
    for at in range(2):
        both = [sums[0][:, 128 + at * cut : 128 + (at + 1) * cut], sums[1][:, at * rest : (at + 1) * rest]]
        both = jnp.concatenate(both, axis=1) * scale
        shares.append(silu(both[:, :width]) * both[:, width:])
    hid0[p, q] = jnp.concatenate(shares, axis=1).astype(BF16)

    def gather(layer, hid, between):
        pieces = {}

        def spread(e):
            at = hid.at[p, lax.rem(q + n - e, n)]
            for d in far_first(n):
                pieces[e, d] = send(at, at, sp.at[layer, e, d - 1], rp.at[layer, e, d - 1], p_peer(d))

        at = hid.at[p, q]
        across = {d: send(at, at, sq.at[layer, d - 1], rq.at[layer, d - 1], q_peer(d)) for d in far_first(n)}
        spread(0)
        for d in near_first(n):
            across[d].wait_recv()
            spread(d)
        between()
        for copy in down_loads[layer]:
            copy.wait()
        for copy in from_other[layer]:
            copy.wait_recv()
        for e in [0] + near_first(n):
            for d in near_first(n):
                pieces[e, d].wait_recv()

    def sum_along_z(layer, product, before, between):
        part[layer] = product.reshape(nz, zrows, depth)
        copies = {}
        for d in far_first(nz):
            send3[layer, d - 1] = part[layer, lax.rem(z + d, nz)].astype(BF16)
            copies[d] = send(
                send3.at[layer, d - 1], recv3.at[layer, d - 1], sz.at[layer, d - 1], rz.at[layer, d - 1], z_peer(d)
            )
        between()
        branch = KEEP * before.astype(F32) + part[layer, z]
        for d in near_first(nz):
            copies[d].wait_recv()
            branch = branch + recv3[layer, d - 1].astype(F32)
        return branch.astype(BF16)

    def nothing():
        return None

    gather(0, hid0, (lambda: deal_parts((0, 1)[: early], True)) if early else nothing)
    product = jnp.dot(hid0[...].reshape(half, 2 * width), down0[...].reshape(2 * width, depth), preferred_element_type=F32)
    before = tokens[pl.ds(pl.multiple_of(c * half + z * zrows, zrows), zrows)]
    stream[0, z] = sum_along_z(0, product, before, lambda: deal_parts((0, 1)[early:], True))

    arriving = {}

    def pass_on(e):
        k = lax.rem(z + nz - e, nz)
        for d in far_first(n):
            arriving[e, d] = send(stream.at[0, k], stream.at[d, k], ss.at[e, d], rs.at[e, d], p_peer(d))

    def normalize(d, k):
        mine = stream[d, k].astype(F32)
        nbuf[k, :, d * depth : (d + 1) * depth] = (mine * gains[d, 1:2]).astype(BF16)
        mine = mine * mine
        parts = mine[:, :128]
        for b in range(1, depth // 128):
            parts = parts + mine[:, b * 128 : (b + 1) * 128]
        squares[d, k] = parts

    at = stream.at[0, z]
    along = {d: send(at, at, ss.at[d, 0], rs.at[d, 0], z_peer(d)) for d in far_first(nz)}
    pass_on(0)
    for e in near_first(nz):
        along[e].wait_recv()
        pass_on(e)
    for k in range(nz):
        normalize(0, k)
    for d in far_first(n):
        copy_to(gains.at[0], gains.at[d], gs.at[d - 1], gr.at[d - 1], p_peer(d)).wait_recv()
    for e in [0] + near_first(nz):
        for d in near_first(n):
            arriving[e, d].wait_recv()
            normalize(d, lax.rem(z + nz - e, nz))
    for d in range(n):
        for k in range(2):
            pltpu.make_async_copy(wg.at[1, pl.ds(0, pw)], w1.at[d, pl.ds(k * pw, pw)], wr.at[d, k]).wait()
    product = 0.0
    for e in range(n):
        normed = nbuf[:, :, e * depth : (e + 1) * depth].reshape(half, depth)
        product = product + lax.dot_general(normed, w1[e], OVER_LAST, preferred_element_type=F32)
    parts = squares[0]
    for d in range(1, n):
        parts = parts + squares[d]
    total = jnp.sum(parts.reshape(half, 128), axis=1, keepdims=True)
    own4[:, :, :edge] = product[:, :edge].reshape(n, group, edge)
    own4[:, :, edge:] = (product[:, edge:] + in_tile(total, 0.0)).reshape(n, group, 128)
    send4[:, :, :edge] = product[:, :edge].astype(BF16).reshape(n, group, edge)
    send4[:, :, edge:] = (product[:, edge:] + two_parts(total)).astype(BF16).reshape(n, group, 128)
    third = {
        d: send(send4.at[lax.rem(q + d, n)], recv4.at[d - 1], s4.at[d - 1], r4.at[d - 1], q_peer(d)) for d in far_first(n)
    }
    total = own4[q]
    for d in near_first(n):
        third[d].wait_recv()
        total = total + recv4[d - 1].astype(F32)
    both = total * lax.rsqrt(all_squares(total[:, edge:]) / features + EPSILON)
    hid1[p, q] = (silu(both[:, :pw]) * both[:, pw : 2 * pw]).astype(BF16)
    gather(1, hid1, nothing)
    product = 0.0
    for e in range(n):
        product = product + jnp.dot(hid1[e].reshape(half, pw), down1[e], preferred_element_type=F32)
    out[c * nz + z] = sum_along_z(1, product, stream[0, z], nothing)
    mine = out.at[c * nz + z]
    rest = {d: send(mine, mine, so.at[0, d - 1], ro.at[0, d - 1], z_peer(d)) for d in far_first(nz)}
    passed = [send(mine, mine, so.at[1, nz - 1], ro.at[1, nz - 1], other)]
    for d in near_first(nz):
        rest[d].wait_recv()
        at = out.at[c * nz + lax.rem(z + nz - d, nz)]
        passed.append(send(at, at, so.at[1, d - 1], ro.at[1, d - 1], other))
    for copy in passed:
        copy.wait_recv()
    for copy in pending:
        copy.wait_send()
    deal_parts((0, 1), False)


def first_cut(width):
    return pl.cdiv(2 * width, 256) * 128


def silu(v):
    return v / (1.0 + jnp.exp(-v))


EARLY = 0


def solution(mesh):
    nz = mesh.shape["cb"] // 2
    n = 4 if mesh.shape["ra"] == 16 else 2
    torus = Mesh(mesh.devices.reshape(n, n, nz, 2), ("y", "x", "z", "c"))
    ra, cb = ("y", "x"), ("z", "c")

    def body(tokens, norm_gain, gate_weight, up_weight, down_weight):
        count, depth = tokens.shape
        width = gate_weight.shape[2]
        pw = width * 2 // n
        half = count // 2
        group, zrows = half // n, half // nz
        wide = pl.cdiv(2 * pw + 64, 128) * 128
        dma = pltpu.SemaphoreType.DMA
        rows = group // n
        cols = 128 + 2 * width
        scratch = [
            pltpu.VMEM((count, depth), BF16),
            pltpu.VMEM((n, nz, zrows, depth), BF16),
            pltpu.VMEM((n, LAYERS, depth), F32),
            pltpu.VMEM((2 * width, depth), BF16),
            pltpu.VMEM((2, width, depth), BF16),
            pltpu.VMEM((n, wide, depth), BF16),
            pltpu.VMEM((n, pw, depth), BF16),
            pltpu.VMEM((nz, zrows, n * depth), BF16),
            pltpu.VMEM((n, nz, zrows, 128), F32),
            pltpu.VMEM((n, group, cols), F32),
            pltpu.VMEM((2, n, group, cols), BF16),
            pltpu.VMEM((2, n, group, cols), BF16),
            pltpu.VMEM((rows, 2 * cols - 128), F32),
            *[pltpu.VMEM((n - 1, rows, 2 * cols - 128), BF16)] * 2,
            pltpu.VMEM((n, n, rows, 2 * width), BF16),
            pltpu.VMEM((n, group, wide), F32),
            pltpu.VMEM((n, group, wide), BF16),
            pltpu.VMEM((n - 1, group, wide), BF16),
            pltpu.VMEM((n, n, group, pw), BF16),
            pltpu.VMEM((LAYERS, nz, zrows, depth), F32),
            *[pltpu.VMEM((LAYERS, nz - 1, zrows, depth), BF16)] * 2,
            dma((5 + n // 2,)),
            *[dma((n - 1,))] * 2,
            dma((2, n // 2, 2)),
            dma((n, 2)),
            *[dma((1 + n // 2,))] * 2,
            *[dma((2, 2, n))] * 2,
            *[dma((2, n - 1))] * 2,
            *[dma((n - 1,))] * 2,
            *[dma((LAYERS, n - 1))] * 2,
            *[dma((LAYERS, n, n - 1))] * 2,
            *[dma((LAYERS, nz - 1))] * 2,
            *[dma((nz, n))] * 2,
            *[dma((2, nz))] * 2,
        ]
        result = pl.pallas_call(
            functools.partial(kernel, n, nz, depth * n * n, EARLY),
            out_shape=jax.ShapeDtypeStruct((2 * nz, zrows, depth), BF16),
            in_specs=[pl.BlockSpec(memory_space=pl.ANY)] * 5,
            out_specs=pl.BlockSpec(memory_space=pltpu.VMEM),
            scratch_shapes=scratch,
            compiler_params=pltpu.CompilerParams(
                collective_id=0, has_side_effects=True, vmem_limit_bytes=60 * 1024 * 1024
            ),
        )(tokens, norm_gain, jnp.swapaxes(gate_weight, 1, 2), jnp.swapaxes(up_weight, 1, 2), down_weight)
        return result.reshape(count, depth)

    in_specs = (P(None, ra), P(None, ra), P(None, ra, cb), P(None, ra, cb), P(None, cb, ra))
    return jax.shard_map(body, mesh=torus, in_specs=in_specs, out_specs=P(None, ra), check_vma=False)
```

```python
import functools

import jax
import jax.numpy as jnp
from jax import lax
from jax.experimental import pallas as pl
from jax.experimental.pallas import tpu as pltpu
from jax.sharding import Mesh
from jax.sharding import PartitionSpec as P

MESH = pl.DeviceIdType.MESH
LAYERS = 2
EPSILON = 1e-06
KEEP = 0.5
F32 = jnp.float32
BF16 = jnp.bfloat16
OVER_LAST = (((1,), (1,)), ((), ()))


def far_first(n):
    return sorted(range(1, n), key=lambda d: (-min(d, n - d), d))


def near_first(n):
    return far_first(n)[::-1]


def kernel(n, nz, features, tok, gain, wg, wu, wd, out, *scratch):
    (
        tokens, stream, gains, w0, down0, w1, down1, nbuf, squares, own1, send1, recv1, own2, send2, recv2, hid0,
        own4, send4, recv4, hid1, part, send3, recv3, fresh,
        staged, load_sem, gs, gr, ws, wr, ds, dr, s1, r1, s2, r2, s4, r4, sq, rq, sp, rp, sz, rz, ss, rs, so, ro,
    ) = scratch
    y, x, z, c = (lax.axis_index(a) for a in ("y", "x", "z", "c"))
    _, _, zrows, depth = stream.shape
    half = nz * zrows
    group = half // n
    rows = group // n
    slices = nz // n
    width = wg.shape[1]
    pw = down1.shape[1]
    wide = w1.shape[1]
    halves = n // 2
    cut = first_cut(width)
    p = c * x + (1 - c) * y
    q = c * y + (1 - c) * x

    def p_peer(d):
        return {"y": lax.rem(y + (1 - c) * d, n), "x": lax.rem(x + c * d, n)}

    def q_peer(d):
        return {"y": lax.rem(y + c * d, n), "x": lax.rem(x + (1 - c) * d, n)}

    def z_peer(d):
        return {"z": lax.rem(z + d, nz)}

    other = {"c": 1 - c}
    pending = []

    def copy_to(src, dst, ss, rs, to):
        return pltpu.make_async_remote_copy(src, dst, ss, rs, device_id=to, device_id_type=MESH)

    def send(*where):
        copy = copy_to(*where)
        copy.start()
        pending.append(copy)
        return copy

    barrier = pltpu.get_barrier_semaphore()
    greeted = [p_peer(d) for d in range(1, n)] + [q_peer(d) for d in range(1, n)]
    greeted += [{**peer, "c": 1 - c} for peer in greeted]
    greeted += [z_peer(d) for d in range(1, nz)] + [{**z_peer(d), **other} for d in range(nz)]
    for peer in greeted:
        pl.semaphore_signal(barrier, 1, device_id=peer, device_id_type=MESH)

    loads = [
        pltpu.make_async_copy(gain, gains.at[0], load_sem.at[0]),
        pltpu.make_async_copy(tok, tokens, load_sem.at[1]),
        pltpu.make_async_copy(wg.at[0], w0.at[pl.ds(0, width)], load_sem.at[2]),
        pltpu.make_async_copy(wu.at[0], w0.at[pl.ds(width, width)], load_sem.at[3]),
    ]
    down_loads = [[pltpu.make_async_copy(wd.at[0], down0.at[0], load_sem.at[4])], [
        pltpu.make_async_copy(wd.at[1, pl.ds(h * pw, pw)], down1.at[c * halves + h], load_sem.at[5 + h])
        for h in range(halves)
    ]]
    part_loads = [
        pltpu.make_async_copy(w.at[1], staged.at[k], load_sem.at[5 + halves + k]) for k, w in enumerate((wg, wu))
    ]
    for copy in loads + down_loads[0] + down_loads[1] + part_loads:
        copy.start()
    w1[:, 2 * pw :, :] = jnp.zeros((n, wide - 2 * pw, depth), BF16)

    lane = lax.broadcasted_iota(jnp.int32, (1, 128), 1)
    edge = wide - 128

    def in_tile(high, low):
        return jnp.where(lane < 64, 0.0, jnp.where(lane < 96, high, low))

    def two_parts(total):
        high = total.astype(BF16).astype(F32)
        return in_tile(high, total - high)

    def all_squares(tile):
        return tile[:, 64:65] + tile[:, 96:97]

    for copy in loads:
        copy.wait()
    for at in range(2):
        mine = tokens[pl.ds((c if at == 0 else 1 - c) * half, half)].astype(F32)
        normed = (mine * gains[0, 0:1]).astype(BF16)
        product = lax.dot_general(normed, w0[...], OVER_LAST, preferred_element_type=F32)
        send1[at, :, :, 128:] = product.astype(BF16).reshape(n, group, 2 * width)
        if at == 0:
            own1[:, :, 128:] = product.reshape(n, group, 2 * width)
            total = jnp.sum(mine * mine, axis=1, keepdims=True)
            own1[:, :, :128] = in_tile(total, 0.0).reshape(n, group, 128)
            send1[0, :, :, :128] = two_parts(total).astype(BF16).reshape(n, group, 128)
    for copy in part_loads:
        copy.wait()
    pl.semaphore_wait(barrier, len(greeted))

    spans = [[pl.ds(0, 128 + cut), pl.ds(128 + cut, 2 * width - cut)], [pl.ds(128, cut), pl.ds(128 + cut, 2 * width - cut)]]
    first = {}
    for piece in range(2):
        for d in far_first(n) + [0]:
            for at in range(2):
                if at == 0 and d == 0:
                    continue
                to = lax.rem((p, q)[at] + d, n)
                first[piece, at, d] = send(
                    send1.at[at, to, :, spans[at][piece]],
                    recv1.at[at, d, :, spans[at][piece]],
                    s1.at[piece, at, d],
                    r1.at[piece, at, d],
                    {**(p_peer, q_peer)[at](d), "c": (c, 1 - c)[at]},
                )
    for d in far_first(n):
        send(gains.at[0], gains.at[d], gs.at[d - 1], gr.at[d - 1], p_peer(d))
    from_other = [[send(wd.at[0], down0.at[1], ds.at[0], dr.at[0], other)], [
        send(wd.at[1, pl.ds(h * pw, pw)], down1.at[c * halves + h], ds.at[1 + h], dr.at[1 + h], other)
        for h in range(halves)
    ]]

    def deal_parts(point, start=True):
        for t in range(2):
            a = x if t else y
            for h in range(halves):
                owner = c * halves + h
                d = lax.rem(owner - a + n, n)
                to = {"x" if t else "y": owner, "c": t}
                here = jnp.logical_and(c == t, owner == a)
                for k in range(2):
                    if start and DEAL[2 * k + h % 2] != point:
                        continue
                    src = staged.at[k, pl.ds(h * pw, pw)]
                    dst = w1.at[d, pl.ds(k * pw, pw)]
                    sem = ws.at[t, h, k]

                    @pl.when(jnp.logical_and(here, start))
                    def _():
                        pltpu.make_async_copy((wg, wu)[k].at[1, pl.ds(h * pw, pw)], dst, wr.at[d, k]).start()

                    @pl.when(jnp.logical_not(here))
                    def _():
                        copy = copy_to(src, dst, sem, wr.at[d, k], to)
                        if start:
                            copy.start()
                        else:
                            copy.wait_send()

    second = {}
    bounds = [0, 128 + 2 * cut, 128 + 4 * width]
    for piece in range(2):
        for d in near_first(n) + [0]:
            for at in range(2):
                if at == 1 or d:
                    first[piece, at, d].wait_recv()
        for d in far_first(n) + [0]:
            at = pl.ds(pl.multiple_of(lax.rem(q + d, n) * rows, rows), rows)
            mine = own1[p, at, spans[0][piece]]
            for e in range(1, n):
                mine = mine + recv1[0, e, at, spans[0][piece]].astype(F32)
            theirs = recv1[1, 0, at, spans[1][piece]].astype(F32)
            for e in range(1, n):
                theirs = theirs + recv1[1, e, at, spans[1][piece]].astype(F32)
            total = [mine, theirs]
            if piece == 0:
                norm = all_squares(mine[:, :128])
                tile = two_parts(norm) if d else in_tile(norm, 0.0)
                total = [tile, mine[:, 128:], theirs]
            total = jnp.concatenate(total, axis=1)
            span = pl.ds(bounds[piece], bounds[piece + 1] - bounds[piece])
            if d == 0:
                own2[:, span] = total
            else:
                send2[d - 1, :, span] = total.astype(BF16)
                second[piece, d] = send(
                    send2.at[d - 1, :, span], recv2.at[d - 1, :, span],
                    s2.at[piece, d - 1], r2.at[piece, d - 1], q_peer(d),
                )
    deal_parts("r")
    sums = []
    for piece in range(2):
        span = pl.ds(bounds[piece], bounds[piece + 1] - bounds[piece])
        total = own2[:, span]
        for d in near_first(n):
            second[piece, d].wait_recv()
            total = total + recv2[d - 1, :, span].astype(F32)
        sums.append(total)
    scale = lax.rsqrt(all_squares(sums[0][:, :128]) / features + EPSILON)
    rest = 2 * width - cut
    shares = []
    for at in range(2):
        both = [sums[0][:, 128 + at * cut : 128 + (at + 1) * cut], sums[1][:, at * rest : (at + 1) * rest]]
        both = jnp.concatenate(both, axis=1) * scale
        shares.append(silu(both[:, :width]) * both[:, width:])
    hid0[p, q] = jnp.concatenate(shares, axis=1).astype(BF16)

    def gather(layer, hid, between, after):
        pieces = {}

        def spread(e):
            at = hid.at[p, lax.rem(q + n - e, n)]
            for d in far_first(n):
                pieces[e, d] = send(at, at, sp.at[layer, e, d - 1], rp.at[layer, e, d - 1], p_peer(d))

        at = hid.at[p, q]
        across = {d: send(at, at, sq.at[layer, d - 1], rq.at[layer, d - 1], q_peer(d)) for d in far_first(n)}
        spread(0)
        between()
        for d in near_first(n):
            across[d].wait_recv()
            spread(d)
        after()
        for copy in down_loads[layer]:
            copy.wait()
        for copy in from_other[layer]:
            copy.wait_recv()
        for e in [0] + near_first(n):
            for d in near_first(n):
                pieces[e, d].wait_recv()

    def sum_along_z(layer, product, before, between):
        part[layer] = product.reshape(nz, zrows, depth)
        copies = {}
        for d in far_first(nz):
            send3[layer, d - 1] = part[layer, lax.rem(z + d, nz)].astype(BF16)
            copies[d] = send(
                send3.at[layer, d - 1], recv3.at[layer, d - 1], sz.at[layer, d - 1], rz.at[layer, d - 1], z_peer(d)
            )
        between()
        branch = KEEP * before.astype(F32) + part[layer, z]
        for d in near_first(nz):
            copies[d].wait_recv()
            branch = branch + recv3[layer, d - 1].astype(F32)
        return branch.astype(BF16)

    def nothing():
        return None

    gather(0, hid0, lambda: deal_parts("q"), lambda: deal_parts("p"))
    product = jnp.dot(hid0[...].reshape(half, 2 * width), down0[...].reshape(2 * width, depth), preferred_element_type=F32)
    before = tokens[pl.ds(pl.multiple_of(c * half + z * zrows, zrows), zrows)]
    fresh[...] = sum_along_z(0, product, before, lambda: deal_parts("z"))
    deal_parts("zz")

    arriving = {}

    def pass_on(e):
        k = lax.rem(z + nz - e, nz)
        for d in far_first(n):
            arriving[e, d] = send(stream.at[0, k], stream.at[d, k], ss.at[e, d], rs.at[e, d], p_peer(d))

    def normalize(d, k):
        mine = stream[d, k].astype(F32)
        nbuf[k, :, d * depth : (d + 1) * depth] = (mine * gains[d, 1:2]).astype(BF16)
        mine = mine * mine
        parts = mine[:, :128]
        for b in range(1, depth // 128):
            parts = parts + mine[:, b * 128 : (b + 1) * 128]
        squares[d, k] = parts

    along = {
        d: send(fresh, stream.at[0, z], ss.at[d, 0], rs.at[d, 0], {**z_peer(d), **other}) for d in far_first(nz) + [0]
    }
    for e in [0] + near_first(nz):
        along[e].wait_recv()
        pass_on(e)
    for k in range(nz):
        normalize(0, k)
    for d in far_first(n):
        copy_to(gains.at[0], gains.at[d], gs.at[d - 1], gr.at[d - 1], p_peer(d)).wait_recv()
    for e in [0] + near_first(nz):
        for d in near_first(n):
            arriving[e, d].wait_recv()
            normalize(d, lax.rem(z + nz - e, nz))
    for d in range(n):
        for k in range(2):
            pltpu.make_async_copy(wg.at[1, pl.ds(0, pw)], w1.at[d, pl.ds(k * pw, pw)], wr.at[d, k]).wait()
    product = 0.0
    for e in range(n):
        normed = nbuf[:, :, e * depth : (e + 1) * depth].reshape(half, depth)
        product = product + lax.dot_general(normed, w1[e], OVER_LAST, preferred_element_type=F32)
    parts = squares[0]
    for d in range(1, n):
        parts = parts + squares[d]
    total = jnp.sum(parts.reshape(half, 128), axis=1, keepdims=True)
    own4[:, :, :edge] = product[:, :edge].reshape(n, group, edge)
    own4[:, :, edge:] = (product[:, edge:] + in_tile(total, 0.0)).reshape(n, group, 128)
    send4[:, :, :edge] = product[:, :edge].astype(BF16).reshape(n, group, edge)
    send4[:, :, edge:] = (product[:, edge:] + two_parts(total)).astype(BF16).reshape(n, group, 128)
    third = {
        d: send(send4.at[lax.rem(q + d, n)], recv4.at[d - 1], s4.at[d - 1], r4.at[d - 1], q_peer(d)) for d in far_first(n)
    }
    total = own4[q]
    for d in near_first(n):
        third[d].wait_recv()
        total = total + recv4[d - 1].astype(F32)
    both = total * lax.rsqrt(all_squares(total[:, edge:]) / features + EPSILON)
    hid1[p, q] = (silu(both[:, :pw]) * both[:, pw : 2 * pw]).astype(BF16)
    gather(1, hid1, nothing, nothing)
    product = 0.0
    for e in range(n):
        product = product + jnp.dot(hid1[e].reshape(half, pw), down1[e], preferred_element_type=F32)
    out[(1 - c) * nz + z] = sum_along_z(1, product, stream[0, z], nothing)
    mine = out.at[(1 - c) * nz + z]
    rest = {d: send(mine, mine, so.at[0, d - 1], ro.at[0, d - 1], z_peer(d)) for d in far_first(nz)}
    passed = [send(mine, mine, so.at[1, nz - 1], ro.at[1, nz - 1], other)]
    for d in near_first(nz):
        rest[d].wait_recv()
        at = out.at[(1 - c) * nz + lax.rem(z + nz - d, nz)]
        passed.append(send(at, at, so.at[1, d - 1], ro.at[1, d - 1], other))
    for copy in passed:
        copy.wait_recv()
    for copy in pending:
        copy.wait_send()
    deal_parts(None, False)


def first_cut(width):
    return pl.cdiv(2 * width, 256) * 128


def silu(v):
    return v / (1.0 + jnp.exp(-v))


DEAL = ('p', 'p', 'z', 'z')


def solution(mesh):
    nz = mesh.shape["cb"] // 2
    n = 4 if mesh.shape["ra"] == 16 else 2
    torus = Mesh(mesh.devices.reshape(n, n, nz, 2), ("y", "x", "z", "c"))
    ra, cb = ("y", "x"), ("z", "c")

    def body(tokens, norm_gain, gate_weight, up_weight, down_weight):
        count, depth = tokens.shape
        width = gate_weight.shape[2]
        pw = width * 2 // n
        half = count // 2
        group, zrows = half // n, half // nz
        wide = pl.cdiv(2 * pw + 64, 128) * 128
        dma = pltpu.SemaphoreType.DMA
        rows = group // n
        cols = 128 + 2 * width
        scratch = [
            pltpu.VMEM((count, depth), BF16),
            pltpu.VMEM((n, nz, zrows, depth), BF16),
            pltpu.VMEM((n, LAYERS, depth), F32),
            pltpu.VMEM((2 * width, depth), BF16),
            pltpu.VMEM((2, width, depth), BF16),
            pltpu.VMEM((n, wide, depth), BF16),
            pltpu.VMEM((n, pw, depth), BF16),
            pltpu.VMEM((nz, zrows, n * depth), BF16),
            pltpu.VMEM((n, nz, zrows, 128), F32),
            pltpu.VMEM((n, group, cols), F32),
            pltpu.VMEM((2, n, group, cols), BF16),
            pltpu.VMEM((2, n, group, cols), BF16),
            pltpu.VMEM((rows, 2 * cols - 128), F32),
            *[pltpu.VMEM((n - 1, rows, 2 * cols - 128), BF16)] * 2,
            pltpu.VMEM((n, n, rows, 2 * width), BF16),
            pltpu.VMEM((n, group, wide), F32),
            pltpu.VMEM((n, group, wide), BF16),
            pltpu.VMEM((n - 1, group, wide), BF16),
            pltpu.VMEM((n, n, group, pw), BF16),
            pltpu.VMEM((LAYERS, nz, zrows, depth), F32),
            *[pltpu.VMEM((LAYERS, nz - 1, zrows, depth), BF16)] * 2,
            pltpu.VMEM((zrows, depth), BF16),
            pltpu.VMEM((2, width, depth), BF16),
            dma((7 + n // 2,)),
            *[dma((n - 1,))] * 2,
            dma((2, n // 2, 2)),
            dma((n, 2)),
            *[dma((1 + n // 2,))] * 2,
            *[dma((2, 2, n))] * 2,
            *[dma((2, n - 1))] * 2,
            *[dma((n - 1,))] * 2,
            *[dma((LAYERS, n - 1))] * 2,
            *[dma((LAYERS, n, n - 1))] * 2,
            *[dma((LAYERS, nz - 1))] * 2,
            *[dma((nz, n))] * 2,
            *[dma((2, nz))] * 2,
        ]
        result = pl.pallas_call(
            functools.partial(kernel, n, nz, depth * n * n),
            out_shape=jax.ShapeDtypeStruct((2 * nz, zrows, depth), BF16),
            in_specs=[pl.BlockSpec(memory_space=pl.ANY)] * 5,
            out_specs=pl.BlockSpec(memory_space=pltpu.VMEM),
            scratch_shapes=scratch,
            compiler_params=pltpu.CompilerParams(
                collective_id=0, has_side_effects=True, vmem_limit_bytes=60 * 1024 * 1024
            ),
        )(tokens, norm_gain, jnp.swapaxes(gate_weight, 1, 2), jnp.swapaxes(up_weight, 1, 2), down_weight)
        return result.reshape(count, depth)

    in_specs = (P(None, ra), P(None, ra), P(None, ra, cb), P(None, ra, cb), P(None, cb, ra))
    return jax.shard_map(body, mesh=torus, in_specs=in_specs, out_specs=P(None, ra), check_vma=False)
```

```python
import functools

import jax
import jax.numpy as jnp
from jax import lax
from jax.experimental import pallas as pl
from jax.experimental.pallas import tpu as pltpu
from jax.sharding import Mesh
from jax.sharding import PartitionSpec as P

MESH = pl.DeviceIdType.MESH
LAYERS = 2
EPSILON = 1e-06
KEEP = 0.5
F32 = jnp.float32
BF16 = jnp.bfloat16
OVER_LAST = (((1,), (1,)), ((), ()))


def far_first(n):
    return sorted(range(1, n), key=lambda d: (-min(d, n - d), d))


def near_first(n):
    return far_first(n)[::-1]


def kernel(n, nz, features, tok, gain, wg, wu, wd, out, *scratch):
    (
        tokens, stream, gains, w0, down0, w1, down1, nbuf, squares, own1, send1, recv1, own2, send2, recv2, hid0,
        own4, send4, recv4, hid1, part, send3, recv3, fresh,
        staged, load_sem, gs, gr, ws, wr, ds, dr, s1, r1, s2, r2, s4, r4, sq, rq, sp, rp, sz, rz, ss, rs, so, ro,
    ) = scratch
    y, x, z, c = (lax.axis_index(a) for a in ("y", "x", "z", "c"))
    _, _, _, zrows, depth = stream.shape
    chunk = nz * zrows
    half = CHUNKS * chunk
    group = half // n
    rows = group // n
    share = chunk // n
    width = wg.shape[1]
    pw = down1.shape[1]
    wide = w1.shape[1]
    halves = n // 2
    cut = first_cut(width)
    p = c * x + (1 - c) * y
    q = c * y + (1 - c) * x

    def p_peer(d):
        return {"y": lax.rem(y + (1 - c) * d, n), "x": lax.rem(x + c * d, n)}

    def q_peer(d):
        return {"y": lax.rem(y + c * d, n), "x": lax.rem(x + (1 - c) * d, n)}

    def z_peer(d):
        return {"z": lax.rem(z + d, nz)}

    other = {"c": 1 - c}
    pending = []

    def copy_to(src, dst, ss, rs, to):
        return pltpu.make_async_remote_copy(src, dst, ss, rs, device_id=to, device_id_type=MESH)

    def send(*where):
        copy = copy_to(*where)
        copy.start()
        pending.append(copy)
        return copy

    barrier = pltpu.get_barrier_semaphore()
    greeted = [p_peer(d) for d in range(1, n)] + [q_peer(d) for d in range(1, n)]
    greeted += [{**peer, "c": 1 - c} for peer in greeted]
    greeted += [z_peer(d) for d in range(1, nz)] + [{**z_peer(d), **other} for d in range(nz)]
    for peer in greeted:
        pl.semaphore_signal(barrier, 1, device_id=peer, device_id_type=MESH)

    loads = [
        pltpu.make_async_copy(gain, gains.at[0], load_sem.at[0]),
        pltpu.make_async_copy(tok, tokens, load_sem.at[1]),
        pltpu.make_async_copy(wg.at[0], w0.at[pl.ds(0, width)], load_sem.at[2]),
        pltpu.make_async_copy(wu.at[0], w0.at[pl.ds(width, width)], load_sem.at[3]),
    ]
    down_loads = [[pltpu.make_async_copy(wd.at[0], down0.at[0], load_sem.at[4])], [
        pltpu.make_async_copy(wd.at[1, pl.ds(h * pw, pw)], down1.at[c * halves + h], load_sem.at[5 + h])
        for h in range(halves)
    ]]
    part_loads = [
        pltpu.make_async_copy(w.at[1], staged.at[k], load_sem.at[5 + halves + k]) for k, w in enumerate((wg, wu))
    ]
    for copy in loads + down_loads[0] + down_loads[1] + part_loads:
        copy.start()
    w1[:, 2 * pw :, :] = jnp.zeros((n, wide - 2 * pw, depth), BF16)

    lane = lax.broadcasted_iota(jnp.int32, (1, 128), 1)
    edge = wide - 128

    def in_tile(high, low):
        return jnp.where(lane < 64, 0.0, jnp.where(lane < 96, high, low))

    def two_parts(total):
        high = total.astype(BF16).astype(F32)
        return in_tile(high, total - high)

    def all_squares(tile):
        return tile[:, 64:65] + tile[:, 96:97]

    for copy in loads:
        copy.wait()
    for at in range(2):
        mine = tokens[pl.ds((c if at == 0 else 1 - c) * half, half)].astype(F32)
        normed = (mine * gains[0, 0:1]).astype(BF16)
        product = lax.dot_general(normed, w0[...], OVER_LAST, preferred_element_type=F32)
        send1[at, :, :, 128:] = product.astype(BF16).reshape(n, group, 2 * width)
        if at == 0:
            own1[:, :, 128:] = product.reshape(n, group, 2 * width)
            total = jnp.sum(mine * mine, axis=1, keepdims=True)
            own1[:, :, :128] = in_tile(total, 0.0).reshape(n, group, 128)
            send1[0, :, :, :128] = two_parts(total).astype(BF16).reshape(n, group, 128)
    for copy in part_loads:
        copy.wait()
    pl.semaphore_wait(barrier, len(greeted))

    spans = [[pl.ds(0, 128 + cut), pl.ds(128 + cut, 2 * width - cut)], [pl.ds(128, cut), pl.ds(128 + cut, 2 * width - cut)]]
    first = {}
    for piece in range(2):
        for d in far_first(n) + [0]:
            for at in range(2):
                if at == 0 and d == 0:
                    continue
                to = lax.rem((p, q)[at] + d, n)
                first[piece, at, d] = send(
                    send1.at[at, to, :, spans[at][piece]],
                    recv1.at[at, d, :, spans[at][piece]],
                    s1.at[piece, at, d],
                    r1.at[piece, at, d],
                    {**(p_peer, q_peer)[at](d), "c": (c, 1 - c)[at]},
                )
    for d in far_first(n):
        send(gains.at[0], gains.at[d], gs.at[d - 1], gr.at[d - 1], p_peer(d))
    from_other = [[send(wd.at[0], down0.at[1], ds.at[0], dr.at[0], other)], [
        send(wd.at[1, pl.ds(h * pw, pw)], down1.at[c * halves + h], ds.at[1 + h], dr.at[1 + h], other)
        for h in range(halves)
    ]]

    def deal_parts(point, start=True):
        for t in range(2):
            a = x if t else y
            for h in range(halves):
                owner = c * halves + h
                d = lax.rem(owner - a + n, n)
                to = {"x" if t else "y": owner, "c": t}
                here = jnp.logical_and(c == t, owner == a)
                for k in range(2):
                    if start and DEAL[2 * k + h % 2] != point:
                        continue
                    src = staged.at[k, pl.ds(h * pw, pw)]
                    dst = w1.at[d, pl.ds(k * pw, pw)]
                    sem = ws.at[t, h, k]

                    @pl.when(jnp.logical_and(here, start))
                    def _():
                        pltpu.make_async_copy((wg, wu)[k].at[1, pl.ds(h * pw, pw)], dst, wr.at[d, k]).start()

                    @pl.when(jnp.logical_not(here))
                    def _():
                        copy = copy_to(src, dst, sem, wr.at[d, k], to)
                        if start:
                            copy.start()
                        else:
                            copy.wait_send()

    second = {}
    bounds = [0, 128 + 2 * cut, 128 + 4 * width]
    for piece in range(2):
        for d in near_first(n) + [0]:
            for at in range(2):
                if at == 1 or d:
                    first[piece, at, d].wait_recv()
        for d in far_first(n) + [0]:
            at = pl.ds(pl.multiple_of(lax.rem(q + d, n) * rows, rows), rows)
            mine = own1[p, at, spans[0][piece]]
            for e in range(1, n):
                mine = mine + recv1[0, e, at, spans[0][piece]].astype(F32)
            theirs = recv1[1, 0, at, spans[1][piece]].astype(F32)
            for e in range(1, n):
                theirs = theirs + recv1[1, e, at, spans[1][piece]].astype(F32)
            total = [mine, theirs]
            if piece == 0:
                norm = all_squares(mine[:, :128])
                tile = two_parts(norm) if d else in_tile(norm, 0.0)
                total = [tile, mine[:, 128:], theirs]
            total = jnp.concatenate(total, axis=1)
            span = pl.ds(bounds[piece], bounds[piece + 1] - bounds[piece])
            if d == 0:
                own2[:, span] = total
            else:
                send2[d - 1, :, span] = total.astype(BF16)
                second[piece, d] = send(
                    send2.at[d - 1, :, span], recv2.at[d - 1, :, span],
                    s2.at[piece, d - 1], r2.at[piece, d - 1], q_peer(d),
                )
    deal_parts("r")
    sums = []
    for piece in range(2):
        span = pl.ds(bounds[piece], bounds[piece + 1] - bounds[piece])
        total = own2[:, span]
        for d in near_first(n):
            second[piece, d].wait_recv()
            total = total + recv2[d - 1, :, span].astype(F32)
        sums.append(total)
    scale = lax.rsqrt(all_squares(sums[0][:, :128]) / features + EPSILON)
    rest = 2 * width - cut
    shares = []
    for at in range(2):
        both = [sums[0][:, 128 + at * cut : 128 + (at + 1) * cut], sums[1][:, at * rest : (at + 1) * rest]]
        both = jnp.concatenate(both, axis=1) * scale
        shares.append(silu(both[:, :width]) * both[:, width:])
    hid0[p, q] = jnp.concatenate(shares, axis=1).astype(BF16)

    def gather(hid, semaphores, layer, between, after):
        sq, rq, sp, rp = semaphores
        pieces = {}

        def spread(e):
            at = hid.at[p, lax.rem(q + n - e, n)]
            for d in far_first(n):
                pieces[e, d] = send(at, at, sp.at[e, d - 1], rp.at[e, d - 1], p_peer(d))

        at = hid.at[p, q]
        across = {d: send(at, at, sq.at[d - 1], rq.at[d - 1], q_peer(d)) for d in far_first(n)}
        spread(0)
        between()
        for d in near_first(n):
            yield
            across[d].wait_recv()
            spread(d)
        after()
        yield
        for e in [0] + near_first(n):
            for d in near_first(n):
                pieces[e, d].wait_recv()

    def send_along_z(layer, k, product):
        part[layer, k] = product.reshape(nz, zrows, depth)
        copies = {}
        for d in far_first(nz):
            at = (layer, k, d - 1)
            send3[at] = part[layer, k, lax.rem(z + d, nz)].astype(BF16)
            copies[d] = send(send3.at[at], recv3.at[at], sz.at[at], rz.at[at], z_peer(d))
        return copies

    def sum_along_z(layer, k, copies, before):
        branch = KEEP * before.astype(F32) + part[layer, k, z]
        for d in near_first(nz):
            copies[d].wait_recv()
            branch = branch + recv3[layer, k, d - 1].astype(F32)
        return branch.astype(BF16)

    def nothing():
        return None

    def wait_down(layer):
        for copy in down_loads[layer]:
            copy.wait()
        for copy in from_other[layer]:
            copy.wait_recv()

    semaphores = [tuple(s.at[k] for s in (sq, rq, sp, rp)) for k in range(1 + CHUNKS)]
    for _ in gather(hid0, semaphores[0], 0, nothing, lambda: deal_parts("p")):
        pass
    wait_down(0)

    def normalize(g, d, k):
        mine = stream[g, d, k].astype(F32)
        nbuf[g, k, :, d * depth : (d + 1) * depth] = (mine * gains[d, 1:2]).astype(BF16)
        mine = mine * mine
        parts = mine[:, :128]
        for b in range(1, depth // 128):
            parts = parts + mine[:, b * 128 : (b + 1) * 128]
        squares[g, d, k] = parts

    def finish(g):
        lines = n // CHUNKS
        units = hid0[g * lines : (g + 1) * lines].reshape(chunk, 2 * width)
        product = jnp.dot(units, down0[...].reshape(2 * width, depth), preferred_element_type=F32)
        copies = send_along_z(0, g, product)
        yield
        before = tokens[pl.ds(pl.multiple_of(c * half + g * chunk + z * zrows, zrows), zrows)]
        fresh[g] = sum_along_z(0, g, copies, before)
        along = {
            d: send(fresh.at[g], stream.at[g, 0, z], ss.at[g, d, 0], rs.at[g, d, 0], {**z_peer(d), **other})
            for d in far_first(nz) + [0]
        }
        arriving = {}
        for e in [0] + near_first(nz):
            yield
            along[e].wait_recv()
            k = lax.rem(z + nz - e, nz)
            for d in far_first(n):
                arriving[e, d] = send(stream.at[g, 0, k], stream.at[g, d, k], ss.at[g, e, d], rs.at[g, e, d], p_peer(d))
        for k in range(nz):
            normalize(g, 0, k)
        if g == 0:
            for d in far_first(n):
                copy_to(gains.at[0], gains.at[d], gs.at[d - 1], gr.at[d - 1], p_peer(d)).wait_recv()
        yield
        for e in [0] + near_first(nz):
            for d in near_first(n):
                arriving[e, d].wait_recv()
                normalize(g, d, lax.rem(z + nz - e, nz))
        if g == 0:
            for d in range(n):
                for k in range(2):
                    pltpu.make_async_copy(wg.at[1, pl.ds(0, pw)], w1.at[d, pl.ds(k * pw, pw)], wr.at[d, k]).wait()
        product = 0.0
        for e in range(n):
            normed = nbuf[g, :, :, e * depth : (e + 1) * depth].reshape(chunk, depth)
            product = product + lax.dot_general(normed, w1[e], OVER_LAST, preferred_element_type=F32)
        parts = squares[g, 0]
        for d in range(1, n):
            parts = parts + squares[g, d]
        total = jnp.sum(parts.reshape(chunk, 128), axis=1, keepdims=True)
        own4[g, :, :, :edge] = product[:, :edge].reshape(n, share, edge)
        own4[g, :, :, edge:] = (product[:, edge:] + in_tile(total, 0.0)).reshape(n, share, 128)
        send4[g, :, :, :edge] = product[:, :edge].astype(BF16).reshape(n, share, edge)
        send4[g, :, :, edge:] = (product[:, edge:] + two_parts(total)).astype(BF16).reshape(n, share, 128)
        third = {
            d: send(send4.at[g, lax.rem(q + d, n)], recv4.at[g, d - 1], s4.at[g, d - 1], r4.at[g, d - 1], q_peer(d))
            for d in far_first(n)
        }
        yield
        total = own4[g, q]
        for d in near_first(n):
            third[d].wait_recv()
            total = total + recv4[g, d - 1].astype(F32)
        both = total * lax.rsqrt(all_squares(total[:, edge:]) / features + EPSILON)
        hid1[g, p, q] = (silu(both[:, :pw]) * both[:, pw : 2 * pw]).astype(BF16)
        yield from gather(hid1.at[g], semaphores[1 + g], 1, nothing, nothing)
        if g == 0:
            wait_down(1)
        product = 0.0
        for e in range(n):
            product = product + jnp.dot(hid1[g, e].reshape(chunk, pw), down1[e], preferred_element_type=F32)
        copies = send_along_z(1, g, product)
        yield
        mine = out.at[1 - c, g, z]
        out[1 - c, g, z] = sum_along_z(1, g, copies, stream[g, 0, z])
        rest = {d: send(mine, mine, so.at[g, 0, d - 1], ro.at[g, 0, d - 1], z_peer(d)) for d in far_first(nz)}
        passed = [send(mine, mine, so.at[g, 1, nz - 1], ro.at[g, 1, nz - 1], other)]
        for d in near_first(nz):
            yield
            rest[d].wait_recv()
            at = out.at[1 - c, g, lax.rem(z + nz - d, nz)]
            passed.append(send(at, at, so.at[g, 1, d - 1], ro.at[g, 1, d - 1], other))
        yield
        for copy in passed:
            copy.wait_recv()

    chunks = [finish(g) for g in range(CHUNKS)]
    for steps in chunks:
        next(steps)
    deal_parts("z")
    while chunks:
        for steps in list(chunks):
            if next(steps, chunks) is chunks:
                chunks.remove(steps)
    for copy in pending:
        copy.wait_send()
    deal_parts(None, False)


def first_cut(width):
    return pl.cdiv(2 * width, 256) * 128


def silu(v):
    return v / (1.0 + jnp.exp(-v))


CHUNKS = 2
DEAL = ('p', 'p', 'z', 'z')


def solution(mesh):
    nz = mesh.shape["cb"] // 2
    n = 4 if mesh.shape["ra"] == 16 else 2
    torus = Mesh(mesh.devices.reshape(n, n, nz, 2), ("y", "x", "z", "c"))
    ra, cb = ("y", "x"), ("z", "c")

    def body(tokens, norm_gain, gate_weight, up_weight, down_weight):
        count, depth = tokens.shape
        width = gate_weight.shape[2]
        pw = width * 2 // n
        half = count // 2
        group, zrows = half // n, half // nz // CHUNKS
        share = group // CHUNKS
        wide = pl.cdiv(2 * pw + 64, 128) * 128
        dma = pltpu.SemaphoreType.DMA
        rows = group // n
        cols = 128 + 2 * width
        scratch = [
            pltpu.VMEM((count, depth), BF16),
            pltpu.VMEM((CHUNKS, n, nz, zrows, depth), BF16),
            pltpu.VMEM((n, LAYERS, depth), F32),
            pltpu.VMEM((2 * width, depth), BF16),
            pltpu.VMEM((2, width, depth), BF16),
            pltpu.VMEM((n, wide, depth), BF16),
            pltpu.VMEM((n, pw, depth), BF16),
            pltpu.VMEM((CHUNKS, nz, zrows, n * depth), BF16),
            pltpu.VMEM((CHUNKS, n, nz, zrows, 128), F32),
            pltpu.VMEM((n, group, cols), F32),
            pltpu.VMEM((2, n, group, cols), BF16),
            pltpu.VMEM((2, n, group, cols), BF16),
            pltpu.VMEM((rows, 2 * cols - 128), F32),
            *[pltpu.VMEM((n - 1, rows, 2 * cols - 128), BF16)] * 2,
            pltpu.VMEM((n, n, rows, 2 * width), BF16),
            pltpu.VMEM((CHUNKS, n, share, wide), F32),
            pltpu.VMEM((CHUNKS, n, share, wide), BF16),
            pltpu.VMEM((CHUNKS, n - 1, share, wide), BF16),
            pltpu.VMEM((CHUNKS, n, n, share, pw), BF16),
            pltpu.VMEM((LAYERS, CHUNKS, nz, zrows, depth), F32),
            *[pltpu.VMEM((LAYERS, CHUNKS, nz - 1, zrows, depth), BF16)] * 2,
            pltpu.VMEM((CHUNKS, zrows, depth), BF16),
            pltpu.VMEM((2, width, depth), BF16),
            dma((7 + n // 2,)),
            *[dma((n - 1,))] * 2,
            dma((2, n // 2, 2)),
            dma((n, 2)),
            *[dma((1 + n // 2,))] * 2,
            *[dma((2, 2, n))] * 2,
            *[dma((2, n - 1))] * 2,
            *[dma((CHUNKS, n - 1))] * 2,
            *[dma((1 + CHUNKS, n - 1))] * 2,
            *[dma((1 + CHUNKS, n, n - 1))] * 2,
            *[dma((LAYERS, CHUNKS, nz - 1))] * 2,
            *[dma((CHUNKS, nz, n))] * 2,
            *[dma((CHUNKS, 2, nz))] * 2,
        ]
        result = pl.pallas_call(
            functools.partial(kernel, n, nz, depth * n * n),
            out_shape=jax.ShapeDtypeStruct((2, CHUNKS, nz, zrows, depth), BF16),
            in_specs=[pl.BlockSpec(memory_space=pl.ANY)] * 5,
            out_specs=pl.BlockSpec(memory_space=pltpu.VMEM),
            scratch_shapes=scratch,
            compiler_params=pltpu.CompilerParams(
                collective_id=0, has_side_effects=True, vmem_limit_bytes=60 * 1024 * 1024
            ),
        )(tokens, norm_gain, jnp.swapaxes(gate_weight, 1, 2), jnp.swapaxes(up_weight, 1, 2), down_weight)
        return result.reshape(count, depth)

    in_specs = (P(None, ra), P(None, ra), P(None, ra, cb), P(None, ra, cb), P(None, cb, ra))
    return jax.shard_map(body, mesh=torus, in_specs=in_specs, out_specs=P(None, ra), check_vma=False)
```

```python
import functools

import jax
import jax.numpy as jnp
from jax import lax
from jax.experimental import pallas as pl
from jax.experimental.pallas import tpu as pltpu
from jax.sharding import Mesh
from jax.sharding import PartitionSpec as P

MESH = pl.DeviceIdType.MESH
LAYERS = 2
EPSILON = 1e-06
KEEP = 0.5
F32 = jnp.float32
BF16 = jnp.bfloat16
OVER_LAST = (((1,), (1,)), ((), ()))


def far_first(n):
    return sorted(range(1, n), key=lambda d: (-min(d, n - d), d))


def near_first(n):
    return far_first(n)[::-1]


def kernel(n, nz, features, tok, gain, wg, wu, wd, out, *scratch):
    (
        tokens, stream, gains, w0, down0, w1, down1, nbuf, squares, own1, send1, recv1, own2, send2, recv2, hid0,
        own4, send4, recv4, hid1, part, send3, recv3, fresh,
        staged, load_sem, gs, gr, ws, wr, ds, dr, s1, r1, s2, r2, s4, r4, sq, rq, sp, rp, sz, rz, ss, rs, so, ro,
    ) = scratch
    y, x, z, c = (lax.axis_index(a) for a in ("y", "x", "z", "c"))
    _, _, _, zrows, depth = stream.shape
    chunk = nz * zrows
    half = CHUNKS * chunk
    group = half // n
    rows = group // n
    share = chunk // n
    width = wg.shape[1]
    pw = down1.shape[1]
    wide = w1.shape[1]
    halves = n // 2
    cut = first_cut(width)
    p = c * x + (1 - c) * y
    q = c * y + (1 - c) * x

    def p_peer(d):
        return {"y": lax.rem(y + (1 - c) * d, n), "x": lax.rem(x + c * d, n)}

    def q_peer(d):
        return {"y": lax.rem(y + c * d, n), "x": lax.rem(x + (1 - c) * d, n)}

    def z_peer(d):
        return {"z": lax.rem(z + d, nz)}

    other = {"c": 1 - c}
    pending = []

    def copy_to(src, dst, ss, rs, to):
        return pltpu.make_async_remote_copy(src, dst, ss, rs, device_id=to, device_id_type=MESH)

    def send(*where):
        copy = copy_to(*where)
        copy.start()
        pending.append(copy)
        return copy

    barrier = pltpu.get_barrier_semaphore()
    greeted = [p_peer(d) for d in range(1, n)] + [q_peer(d) for d in range(1, n)]
    greeted += [{**peer, "c": 1 - c} for peer in greeted]
    greeted += [z_peer(d) for d in range(1, nz)] + [{**z_peer(d), **other} for d in range(nz)]
    for peer in greeted:
        pl.semaphore_signal(barrier, 1, device_id=peer, device_id_type=MESH)

    loads = [
        pltpu.make_async_copy(gain, gains.at[0], load_sem.at[0]),
        pltpu.make_async_copy(tok, tokens, load_sem.at[1]),
        pltpu.make_async_copy(wg.at[0], w0.at[pl.ds(0, width)], load_sem.at[2]),
        pltpu.make_async_copy(wu.at[0], w0.at[pl.ds(width, width)], load_sem.at[3]),
    ]
    down_loads = [[pltpu.make_async_copy(wd.at[0], down0.at[0], load_sem.at[4])], [
        pltpu.make_async_copy(wd.at[1, pl.ds(h * pw, pw)], down1.at[c * halves + h], load_sem.at[5 + h])
        for h in range(halves)
    ]]
    part_loads = [
        pltpu.make_async_copy(w.at[1], staged.at[k], load_sem.at[5 + halves + k]) for k, w in enumerate((wg, wu))
    ]
    for copy in loads + down_loads[0] + down_loads[1] + part_loads:
        copy.start()
    w1[:, 2 * pw :, :] = jnp.zeros((n, wide - 2 * pw, depth), BF16)

    lane = lax.broadcasted_iota(jnp.int32, (1, 128), 1)
    edge = wide - 128

    def in_tile(high, low):
        return jnp.where(lane < 64, 0.0, jnp.where(lane < 96, high, low))

    def two_parts(total):
        high = total.astype(BF16).astype(F32)
        return in_tile(high, total - high)

    def all_squares(tile):
        return tile[:, 64:65] + tile[:, 96:97]

    for copy in loads:
        copy.wait()
    for at in range(2):
        mine = tokens[pl.ds((c if at == 0 else 1 - c) * half, half)].astype(F32)
        normed = (mine * gains[0, 0:1]).astype(BF16)
        product = lax.dot_general(normed, w0[...], OVER_LAST, preferred_element_type=F32)
        send1[at, :, :, 128:] = product.astype(BF16).reshape(n, group, 2 * width)
        if at == 0:
            own1[:, :, 128:] = product.reshape(n, group, 2 * width)
            total = jnp.sum(mine * mine, axis=1, keepdims=True)
            own1[:, :, :128] = in_tile(total, 0.0).reshape(n, group, 128)
            send1[0, :, :, :128] = two_parts(total).astype(BF16).reshape(n, group, 128)
    for copy in part_loads:
        copy.wait()
    pl.semaphore_wait(barrier, len(greeted))

    spans = [[pl.ds(0, 128 + cut), pl.ds(128 + cut, 2 * width - cut)], [pl.ds(128, cut), pl.ds(128 + cut, 2 * width - cut)]]
    first = {}
    for piece in range(2):
        for d in far_first(n) + [0]:
            for at in range(2):
                if at == 0 and d == 0:
                    continue
                to = lax.rem((p, q)[at] + d, n)
                first[piece, at, d] = send(
                    send1.at[at, to, :, spans[at][piece]],
                    recv1.at[at, d, :, spans[at][piece]],
                    s1.at[piece, at, d],
                    r1.at[piece, at, d],
                    {**(p_peer, q_peer)[at](d), "c": (c, 1 - c)[at]},
                )
    for d in far_first(n):
        send(gains.at[0], gains.at[d], gs.at[d - 1], gr.at[d - 1], p_peer(d))
    from_other = [[send(wd.at[0], down0.at[1], ds.at[0], dr.at[0], other)], [
        send(wd.at[1, pl.ds(h * pw, pw)], down1.at[c * halves + h], ds.at[1 + h], dr.at[1 + h], other)
        for h in range(halves)
    ]]

    def deal_parts(point, start=True):
        for t in range(2):
            a = x if t else y
            for h in range(halves):
                owner = c * halves + h
                d = lax.rem(owner - a + n, n)
                to = {"x" if t else "y": owner, "c": t}
                here = jnp.logical_and(c == t, owner == a)
                for k in range(2):
                    if start and DEAL[2 * k + h % 2] != point:
                        continue
                    src = staged.at[k, pl.ds(h * pw, pw)]
                    dst = w1.at[d, pl.ds(k * pw, pw)]
                    sem = ws.at[t, h, k]

                    @pl.when(jnp.logical_and(here, start))
                    def _():
                        pltpu.make_async_copy((wg, wu)[k].at[1, pl.ds(h * pw, pw)], dst, wr.at[d, k]).start()

                    @pl.when(jnp.logical_not(here))
                    def _():
                        copy = copy_to(src, dst, sem, wr.at[d, k], to)
                        if start:
                            copy.start()
                        else:
                            copy.wait_send()

    second = {}
    bounds = [0, 128 + 2 * cut, 128 + 4 * width]
    for piece in range(2):
        for d in near_first(n) + [0]:
            for at in range(2):
                if at == 1 or d:
                    first[piece, at, d].wait_recv()
        for d in far_first(n) + [0]:
            at = pl.ds(pl.multiple_of(lax.rem(q + d, n) * rows, rows), rows)
            mine = own1[p, at, spans[0][piece]]
            for e in range(1, n):
                mine = mine + recv1[0, e, at, spans[0][piece]].astype(F32)
            theirs = recv1[1, 0, at, spans[1][piece]].astype(F32)
            for e in range(1, n):
                theirs = theirs + recv1[1, e, at, spans[1][piece]].astype(F32)
            total = [mine, theirs]
            if piece == 0:
                norm = all_squares(mine[:, :128])
                tile = two_parts(norm) if d else in_tile(norm, 0.0)
                total = [tile, mine[:, 128:], theirs]
            total = jnp.concatenate(total, axis=1)
            span = pl.ds(bounds[piece], bounds[piece + 1] - bounds[piece])
            if d == 0:
                own2[:, span] = total
            else:
                send2[d - 1, :, span] = total.astype(BF16)
                second[piece, d] = send(
                    send2.at[d - 1, :, span], recv2.at[d - 1, :, span],
                    s2.at[piece, d - 1], r2.at[piece, d - 1], q_peer(d),
                )
    deal_parts("r")
    sums = []
    for piece in range(2):
        span = pl.ds(bounds[piece], bounds[piece + 1] - bounds[piece])
        total = own2[:, span]
        for d in near_first(n):
            second[piece, d].wait_recv()
            total = total + recv2[d - 1, :, span].astype(F32)
        sums.append(total)
    scale = lax.rsqrt(all_squares(sums[0][:, :128]) / features + EPSILON)
    rest = 2 * width - cut
    shares = []
    for at in range(2):
        both = [sums[0][:, 128 + at * cut : 128 + (at + 1) * cut], sums[1][:, at * rest : (at + 1) * rest]]
        both = jnp.concatenate(both, axis=1) * scale
        shares.append(silu(both[:, :width]) * both[:, width:])
    hid0[p, q] = jnp.concatenate(shares, axis=1).astype(BF16)

    def gather(hid, semaphores, layer, between, after):
        sq, rq, sp, rp = semaphores
        pieces = {}

        def spread(e):
            at = hid.at[p, lax.rem(q + n - e, n)]
            for d in far_first(n):
                pieces[e, d] = send(at, at, sp.at[e, d - 1], rp.at[e, d - 1], p_peer(d))

        at = hid.at[p, q]
        across = {d: send(at, at, sq.at[d - 1], rq.at[d - 1], q_peer(d)) for d in far_first(n)}
        spread(0)
        between()
        for d in near_first(n):
            yield
            across[d].wait_recv()
            spread(d)
        after()
        yield
        for e in [0] + near_first(n):
            for d in near_first(n):
                pieces[e, d].wait_recv()

    def send_along_z(layer, k, product):
        part[layer, k] = product.reshape(nz, zrows, depth)
        copies = {}
        for d in far_first(nz):
            at = (layer, k, d - 1)
            send3[at] = part[layer, k, lax.rem(z + d, nz)].astype(BF16)
            copies[d] = send(send3.at[at], recv3.at[at], sz.at[at], rz.at[at], z_peer(d))
        return copies

    def sum_along_z(layer, k, copies, before):
        branch = KEEP * before.astype(F32) + part[layer, k, z]
        for d in near_first(nz):
            copies[d].wait_recv()
            branch = branch + recv3[layer, k, d - 1].astype(F32)
        return branch.astype(BF16)

    def nothing():
        return None

    def wait_down(layer):
        for copy in down_loads[layer]:
            copy.wait()
        for copy in from_other[layer]:
            copy.wait_recv()

    semaphores = [tuple(s.at[k] for s in (sq, rq, sp, rp)) for k in range(1 + CHUNKS)]
    for _ in gather(hid0, semaphores[0], 0, lambda: deal_parts("q"), lambda: deal_parts("p")):
        pass
    wait_down(0)

    def normalize(g, d, k):
        mine = stream[g, d, k].astype(F32)
        nbuf[g, k, :, d * depth : (d + 1) * depth] = (mine * gains[d, 1:2]).astype(BF16)
        mine = mine * mine
        parts = mine[:, :128]
        for b in range(1, depth // 128):
            parts = parts + mine[:, b * 128 : (b + 1) * 128]
        squares[g, d, k] = parts

    def finish(g):
        lines = n // CHUNKS
        units = hid0[g * lines : (g + 1) * lines].reshape(chunk, 2 * width)
        product = jnp.dot(units, down0[...].reshape(2 * width, depth), preferred_element_type=F32)
        copies = send_along_z(0, g, product)
        yield
        before = tokens[pl.ds(pl.multiple_of(c * half + g * chunk + z * zrows, zrows), zrows)]
        fresh[g] = sum_along_z(0, g, copies, before)
        along = {
            d: send(fresh.at[g], stream.at[g, 0, z], ss.at[g, d, 0], rs.at[g, d, 0], {**z_peer(d), **other})
            for d in [0] + near_first(nz)
        }
        arriving = {}
        for e in [0] + near_first(nz):
            yield
            along[e].wait_recv()
            k = lax.rem(z + nz - e, nz)
            for d in far_first(n):
                arriving[e, d] = send(stream.at[g, 0, k], stream.at[g, d, k], ss.at[g, e, d], rs.at[g, e, d], p_peer(d))
        for k in range(nz):
            normalize(g, 0, k)
        if g == 0:
            for d in far_first(n):
                copy_to(gains.at[0], gains.at[d], gs.at[d - 1], gr.at[d - 1], p_peer(d)).wait_recv()
        yield
        for e in [0] + near_first(nz):
            for d in near_first(n):
                arriving[e, d].wait_recv()
                normalize(g, d, lax.rem(z + nz - e, nz))
        if g == 0:
            for d in range(n):
                for k in range(2):
                    pltpu.make_async_copy(wg.at[1, pl.ds(0, pw)], w1.at[d, pl.ds(k * pw, pw)], wr.at[d, k]).wait()
        product = 0.0
        for e in range(n):
            normed = nbuf[g, :, :, e * depth : (e + 1) * depth].reshape(chunk, depth)
            product = product + lax.dot_general(normed, w1[e], OVER_LAST, preferred_element_type=F32)
        parts = squares[g, 0]
        for d in range(1, n):
            parts = parts + squares[g, d]
        total = jnp.sum(parts.reshape(chunk, 128), axis=1, keepdims=True)
        own4[g, :, :, :edge] = product[:, :edge].reshape(n, share, edge)
        own4[g, :, :, edge:] = (product[:, edge:] + in_tile(total, 0.0)).reshape(n, share, 128)
        send4[g, :, :, :edge] = product[:, :edge].astype(BF16).reshape(n, share, edge)
        send4[g, :, :, edge:] = (product[:, edge:] + two_parts(total)).astype(BF16).reshape(n, share, 128)
        third = {
            d: send(send4.at[g, lax.rem(q + d, n)], recv4.at[g, d - 1], s4.at[g, d - 1], r4.at[g, d - 1], q_peer(d))
            for d in far_first(n)
        }
        yield
        total = own4[g, q]
        for d in near_first(n):
            third[d].wait_recv()
            total = total + recv4[g, d - 1].astype(F32)
        both = total * lax.rsqrt(all_squares(total[:, edge:]) / features + EPSILON)
        hid1[g, p, q] = (silu(both[:, :pw]) * both[:, pw : 2 * pw]).astype(BF16)
        yield from gather(hid1.at[g], semaphores[1 + g], 1, nothing, nothing)
        if g == 0:
            wait_down(1)
        product = 0.0
        for e in range(n):
            product = product + jnp.dot(hid1[g, e].reshape(chunk, pw), down1[e], preferred_element_type=F32)
        copies = send_along_z(1, g, product)
        yield
        mine = out.at[1 - c, g, z]
        out[1 - c, g, z] = sum_along_z(1, g, copies, stream[g, 0, z])
        rest = {d: send(mine, mine, so.at[g, 0, d - 1], ro.at[g, 0, d - 1], z_peer(d)) for d in far_first(nz)}
        passed = [send(mine, mine, so.at[g, 1, nz - 1], ro.at[g, 1, nz - 1], other)]
        for d in near_first(nz):
            yield
            rest[d].wait_recv()
            at = out.at[1 - c, g, lax.rem(z + nz - d, nz)]
            passed.append(send(at, at, so.at[g, 1, d - 1], ro.at[g, 1, d - 1], other))
        yield
        for copy in passed:
            copy.wait_recv()

    chunks = [finish(g) for g in range(CHUNKS)]
    for steps in chunks:
        next(steps)
    deal_parts("z")
    while chunks:
        for steps in list(chunks):
            if next(steps, chunks) is chunks:
                chunks.remove(steps)
    for copy in pending:
        copy.wait_send()
    deal_parts(None, False)


def first_cut(width):
    return pl.cdiv(2 * width, 256) * 128


def silu(v):
    return v / (1.0 + jnp.exp(-v))


CHUNKS = 2
DEAL = ('q', 'p', 'z', 'z')


def solution(mesh):
    nz = mesh.shape["cb"] // 2
    n = 4 if mesh.shape["ra"] == 16 else 2
    torus = Mesh(mesh.devices.reshape(n, n, nz, 2), ("y", "x", "z", "c"))
    ra, cb = ("y", "x"), ("z", "c")

    def body(tokens, norm_gain, gate_weight, up_weight, down_weight):
        count, depth = tokens.shape
        width = gate_weight.shape[2]
        pw = width * 2 // n
        half = count // 2
        group, zrows = half // n, half // nz // CHUNKS
        share = group // CHUNKS
        wide = pl.cdiv(2 * pw + 64, 128) * 128
        dma = pltpu.SemaphoreType.DMA
        rows = group // n
        cols = 128 + 2 * width
        scratch = [
            pltpu.VMEM((count, depth), BF16),
            pltpu.VMEM((CHUNKS, n, nz, zrows, depth), BF16),
            pltpu.VMEM((n, LAYERS, depth), F32),
            pltpu.VMEM((2 * width, depth), BF16),
            pltpu.VMEM((2, width, depth), BF16),
            pltpu.VMEM((n, wide, depth), BF16),
            pltpu.VMEM((n, pw, depth), BF16),
            pltpu.VMEM((CHUNKS, nz, zrows, n * depth), BF16),
            pltpu.VMEM((CHUNKS, n, nz, zrows, 128), F32),
            pltpu.VMEM((n, group, cols), F32),
            pltpu.VMEM((2, n, group, cols), BF16),
            pltpu.VMEM((2, n, group, cols), BF16),
            pltpu.VMEM((rows, 2 * cols - 128), F32),
            *[pltpu.VMEM((n - 1, rows, 2 * cols - 128), BF16)] * 2,
            pltpu.VMEM((n, n, rows, 2 * width), BF16),
            pltpu.VMEM((CHUNKS, n, share, wide), F32),
            pltpu.VMEM((CHUNKS, n, share, wide), BF16),
            pltpu.VMEM((CHUNKS, n - 1, share, wide), BF16),
            pltpu.VMEM((CHUNKS, n, n, share, pw), BF16),
            pltpu.VMEM((LAYERS, CHUNKS, nz, zrows, depth), F32),
            *[pltpu.VMEM((LAYERS, CHUNKS, nz - 1, zrows, depth), BF16)] * 2,
            pltpu.VMEM((CHUNKS, zrows, depth), BF16),
            pltpu.VMEM((2, width, depth), BF16),
            dma((7 + n // 2,)),
            *[dma((n - 1,))] * 2,
            dma((2, n // 2, 2)),
            dma((n, 2)),
            *[dma((1 + n // 2,))] * 2,
            *[dma((2, 2, n))] * 2,
            *[dma((2, n - 1))] * 2,
            *[dma((CHUNKS, n - 1))] * 2,
            *[dma((1 + CHUNKS, n - 1))] * 2,
            *[dma((1 + CHUNKS, n, n - 1))] * 2,
            *[dma((LAYERS, CHUNKS, nz - 1))] * 2,
            *[dma((CHUNKS, nz, n))] * 2,
            *[dma((CHUNKS, 2, nz))] * 2,
        ]
        result = pl.pallas_call(
            functools.partial(kernel, n, nz, depth * n * n),
            out_shape=jax.ShapeDtypeStruct((2, CHUNKS, nz, zrows, depth), BF16),
            in_specs=[pl.BlockSpec(memory_space=pl.ANY)] * 5,
            out_specs=pl.BlockSpec(memory_space=pltpu.VMEM),
            scratch_shapes=scratch,
            compiler_params=pltpu.CompilerParams(
                collective_id=0, has_side_effects=True, vmem_limit_bytes=60 * 1024 * 1024
            ),
        )(tokens, norm_gain, jnp.swapaxes(gate_weight, 1, 2), jnp.swapaxes(up_weight, 1, 2), down_weight)
        return result.reshape(count, depth)

    in_specs = (P(None, ra), P(None, ra), P(None, ra, cb), P(None, ra, cb), P(None, cb, ra))
    return jax.shard_map(body, mesh=torus, in_specs=in_specs, out_specs=P(None, ra), check_vma=False)
```

```python
import functools

import jax
import jax.numpy as jnp
from jax import lax
from jax.experimental import pallas as pl
from jax.experimental.pallas import tpu as pltpu
from jax.sharding import Mesh
from jax.sharding import PartitionSpec as P

MESH = pl.DeviceIdType.MESH
LAYERS = 2
EPSILON = 1e-06
KEEP = 0.5
F32 = jnp.float32
BF16 = jnp.bfloat16
OVER_LAST = (((1,), (1,)), ((), ()))


def far_first(n):
    return sorted(range(1, n), key=lambda d: (-min(d, n - d), d))


def near_first(n):
    return far_first(n)[::-1]


def kernel(n, nz, features, tok, gain, wg, wu, wd, out, *scratch):
    (
        tokens, stream, gains, w0, down0, w1, down1, nbuf, squares, own1, send1, recv1, own2, send2, recv2, hid0,
        own4, send4, recv4, hid1, part, send3, recv3, fresh,
        staged, load_sem, gs, gr, ws, wr, ds, dr, s1, r1, s2, r2, s4, r4, sq, rq, sp, rp, sz, rz, ss, rs, so, ro,
    ) = scratch
    y, x, z, c = (lax.axis_index(a) for a in ("y", "x", "z", "c"))
    _, _, _, zrows, depth = stream.shape
    chunk = nz * zrows
    half = CHUNKS * chunk
    group = half // n
    rows = group // n
    share = chunk // n
    width = wg.shape[1]
    pw = down1.shape[1]
    wide = w1.shape[1]
    halves = n // 2
    cut = first_cut(width)
    p = c * x + (1 - c) * y
    q = c * y + (1 - c) * x

    def p_peer(d):
        return {"y": lax.rem(y + (1 - c) * d, n), "x": lax.rem(x + c * d, n)}

    def q_peer(d):
        return {"y": lax.rem(y + c * d, n), "x": lax.rem(x + (1 - c) * d, n)}

    def z_peer(d):
        return {"z": lax.rem(z + d, nz)}

    other = {"c": 1 - c}
    pending = []

    def copy_to(src, dst, ss, rs, to):
        return pltpu.make_async_remote_copy(src, dst, ss, rs, device_id=to, device_id_type=MESH)

    def send(*where):
        copy = copy_to(*where)
        copy.start()
        pending.append(copy)
        return copy

    barrier = pltpu.get_barrier_semaphore()
    greeted = [p_peer(d) for d in range(1, n)] + [q_peer(d) for d in range(1, n)]
    greeted += [{**peer, "c": 1 - c} for peer in greeted]
    greeted += [z_peer(d) for d in range(1, nz)] + [{**z_peer(d), **other} for d in range(nz)]
    for peer in greeted:
        pl.semaphore_signal(barrier, 1, device_id=peer, device_id_type=MESH)

    loads = [
        pltpu.make_async_copy(gain, gains.at[0], load_sem.at[0]),
        pltpu.make_async_copy(tok, tokens, load_sem.at[1]),
        pltpu.make_async_copy(wg.at[0], w0.at[pl.ds(0, width)], load_sem.at[2]),
        pltpu.make_async_copy(wu.at[0], w0.at[pl.ds(width, width)], load_sem.at[3]),
    ]
    down_loads = [[pltpu.make_async_copy(wd.at[0], down0.at[0], load_sem.at[4])], [
        pltpu.make_async_copy(wd.at[1, pl.ds(h * pw, pw)], down1.at[c * halves + h], load_sem.at[5 + h])
        for h in range(halves)
    ]]
    part_loads = [
        pltpu.make_async_copy(w.at[1], staged.at[k], load_sem.at[5 + halves + k]) for k, w in enumerate((wg, wu))
    ]
    for copy in loads + down_loads[0] + down_loads[1] + part_loads:
        copy.start()
    w1[:, 2 * pw :, :] = jnp.zeros((n, wide - 2 * pw, depth), BF16)

    lane = lax.broadcasted_iota(jnp.int32, (1, 128), 1)
    edge = wide - 128

    def in_tile(high, low):
        return jnp.where(lane < 64, 0.0, jnp.where(lane < 96, high, low))

    def two_parts(total):
        high = total.astype(BF16).astype(F32)
        return in_tile(high, total - high)

    def all_squares(tile):
        return tile[:, 64:65] + tile[:, 96:97]

    for copy in loads:
        copy.wait()
    for at in range(2):
        mine = tokens[pl.ds((c if at == 0 else 1 - c) * half, half)].astype(F32)
        normed = (mine * gains[0, 0:1]).astype(BF16)
        product = lax.dot_general(normed, w0[...], OVER_LAST, preferred_element_type=F32)
        send1[at, :, :, 128:] = product.astype(BF16).reshape(n, group, 2 * width)
        if at == 0:
            own1[:, :, 128:] = product.reshape(n, group, 2 * width)
            total = jnp.sum(mine * mine, axis=1, keepdims=True)
            own1[:, :, :128] = in_tile(total, 0.0).reshape(n, group, 128)
            send1[0, :, :, :128] = two_parts(total).astype(BF16).reshape(n, group, 128)
    for copy in part_loads:
        copy.wait()
    pl.semaphore_wait(barrier, len(greeted))

    spans = [[pl.ds(0, 128 + cut), pl.ds(128 + cut, 2 * width - cut)], [pl.ds(128, cut), pl.ds(128 + cut, 2 * width - cut)]]
    first = {}
    for piece in range(2):
        for d in far_first(n) + [0]:
            for at in range(2):
                if at == 0 and d == 0:
                    continue
                to = lax.rem((p, q)[at] + d, n)
                first[piece, at, d] = send(
                    send1.at[at, to, :, spans[at][piece]],
                    recv1.at[at, d, :, spans[at][piece]],
                    s1.at[piece, at, d],
                    r1.at[piece, at, d],
                    {**(p_peer, q_peer)[at](d), "c": (c, 1 - c)[at]},
                )
    for d in far_first(n):
        send(gains.at[0], gains.at[d], gs.at[d - 1], gr.at[d - 1], p_peer(d))
    from_other = [[send(wd.at[0], down0.at[1], ds.at[0], dr.at[0], other)], [
        send(wd.at[1, pl.ds(h * pw, pw)], down1.at[c * halves + h], ds.at[1 + h], dr.at[1 + h], other)
        for h in range(halves)
    ]]

    def deal_parts(point, start=True):
        for t in range(2):
            a = x if t else y
            for h in range(halves):
                owner = c * halves + h
                d = lax.rem(owner - a + n, n)
                to = {"x" if t else "y": owner, "c": t}
                here = jnp.logical_and(c == t, owner == a)
                for k in range(2):
                    if start and DEAL[2 * k + h % 2] != point:
                        continue
                    src = staged.at[k, pl.ds(h * pw, pw)]
                    dst = w1.at[d, pl.ds(k * pw, pw)]
                    sem = ws.at[t, h, k]

                    @pl.when(jnp.logical_and(here, start))
                    def _():
                        pltpu.make_async_copy((wg, wu)[k].at[1, pl.ds(h * pw, pw)], dst, wr.at[d, k]).start()

                    @pl.when(jnp.logical_not(here))
                    def _():
                        copy = copy_to(src, dst, sem, wr.at[d, k], to)
                        if start:
                            copy.start()
                        else:
                            copy.wait_send()

    second = {}
    bounds = [0, 128 + 2 * cut, 128 + 4 * width]
    for piece in range(2):
        for d in near_first(n) + [0]:
            for at in range(2):
                if at == 1 or d:
                    first[piece, at, d].wait_recv()
        for d in far_first(n) + [0]:
            at = pl.ds(pl.multiple_of(lax.rem(q + d, n) * rows, rows), rows)
            mine = own1[p, at, spans[0][piece]]
            for e in range(1, n):
                mine = mine + recv1[0, e, at, spans[0][piece]].astype(F32)
            theirs = recv1[1, 0, at, spans[1][piece]].astype(F32)
            for e in range(1, n):
                theirs = theirs + recv1[1, e, at, spans[1][piece]].astype(F32)
            total = [mine, theirs]
            if piece == 0:
                norm = all_squares(mine[:, :128])
                tile = two_parts(norm) if d else in_tile(norm, 0.0)
                total = [tile, mine[:, 128:], theirs]
            total = jnp.concatenate(total, axis=1)
            span = pl.ds(bounds[piece], bounds[piece + 1] - bounds[piece])
            if d == 0:
                own2[:, span] = total
            else:
                send2[d - 1, :, span] = total.astype(BF16)
                second[piece, d] = send(
                    send2.at[d - 1, :, span], recv2.at[d - 1, :, span],
                    s2.at[piece, d - 1], r2.at[piece, d - 1], q_peer(d),
                )
    deal_parts("r")
    sums = []
    for piece in range(2):
        span = pl.ds(bounds[piece], bounds[piece + 1] - bounds[piece])
        total = own2[:, span]
        for d in near_first(n):
            second[piece, d].wait_recv()
            total = total + recv2[d - 1, :, span].astype(F32)
        sums.append(total)
    scale = lax.rsqrt(all_squares(sums[0][:, :128]) / features + EPSILON)
    rest = 2 * width - cut
    shares = []
    for at in range(2):
        both = [sums[0][:, 128 + at * cut : 128 + (at + 1) * cut], sums[1][:, at * rest : (at + 1) * rest]]
        both = jnp.concatenate(both, axis=1) * scale
        shares.append(silu(both[:, :width]) * both[:, width:])
    hid0[p, q] = jnp.concatenate(shares, axis=1).astype(BF16)

    def gather(hid, semaphores, layer, between, after):
        sq, rq, sp, rp = semaphores
        pieces = {}

        def spread(e):
            at = hid.at[p, lax.rem(q + n - e, n)]
            for d in far_first(n):
                pieces[e, d] = send(at, at, sp.at[e, d - 1], rp.at[e, d - 1], p_peer(d))

        at = hid.at[p, q]
        across = {d: send(at, at, sq.at[d - 1], rq.at[d - 1], q_peer(d)) for d in far_first(n)}
        spread(0)
        between()
        for d in near_first(n):
            yield
            across[d].wait_recv()
            spread(d)
        after()
        yield
        for e in [0] + near_first(n):
            for d in near_first(n):
                pieces[e, d].wait_recv()

    def send_along_z(layer, k, product):
        part[layer, k] = product.reshape(nz, zrows, depth)
        copies = {}
        for d in far_first(nz):
            at = (layer, k, d - 1)
            send3[at] = part[layer, k, lax.rem(z + d, nz)].astype(BF16)
            copies[d] = send(send3.at[at], recv3.at[at], sz.at[at], rz.at[at], z_peer(d))
        return copies

    def sum_along_z(layer, k, copies, before):
        branch = KEEP * before.astype(F32) + part[layer, k, z]
        for d in near_first(nz):
            copies[d].wait_recv()
            branch = branch + recv3[layer, k, d - 1].astype(F32)
        return branch.astype(BF16)

    def nothing():
        return None

    def wait_down(layer):
        for copy in down_loads[layer]:
            copy.wait()
        for copy in from_other[layer]:
            copy.wait_recv()

    semaphores = [tuple(s.at[k] for s in (sq, rq, sp, rp)) for k in range(1 + CHUNKS)]
    for _ in gather(hid0, semaphores[0], 0, lambda: deal_parts("q"), lambda: deal_parts("p")):
        pass
    wait_down(0)

    def normalize(g, d, k):
        mine = stream[g, d, k].astype(F32)
        nbuf[g, k, :, d * depth : (d + 1) * depth] = (mine * gains[d, 1:2]).astype(BF16)
        mine = mine * mine
        parts = mine[:, :128]
        for b in range(1, depth // 128):
            parts = parts + mine[:, b * 128 : (b + 1) * 128]
        squares[g, d, k] = parts

    def finish(g):
        lines = n // CHUNKS
        units = hid0[g * lines : (g + 1) * lines].reshape(chunk, 2 * width)
        product = jnp.dot(units, down0[...].reshape(2 * width, depth), preferred_element_type=F32)
        copies = send_along_z(0, g, product)
        yield
        before = tokens[pl.ds(pl.multiple_of(c * half + g * chunk + z * zrows, zrows), zrows)]
        fresh[g] = sum_along_z(0, g, copies, before)
        along = {
            d: send(fresh.at[g], stream.at[g, 0, z], ss.at[g, d, 0], rs.at[g, d, 0], {**z_peer(d), **other})
            for d in [0] + near_first(nz)
        }
        arriving = {}
        for e in [0] + near_first(nz):
            yield
            along[e].wait_recv()
            k = lax.rem(z + nz - e, nz)
            for d in far_first(n):
                arriving[e, d] = send(stream.at[g, 0, k], stream.at[g, d, k], ss.at[g, e, d], rs.at[g, e, d], p_peer(d))
        for k in range(nz):
            normalize(g, 0, k)
        if g == 0:
            for d in far_first(n):
                copy_to(gains.at[0], gains.at[d], gs.at[d - 1], gr.at[d - 1], p_peer(d)).wait_recv()
        yield
        for e in [0] + near_first(nz):
            for d in near_first(n):
                arriving[e, d].wait_recv()
                normalize(g, d, lax.rem(z + nz - e, nz))
        if g == 0:
            for d in range(n):
                for k in range(2):
                    pltpu.make_async_copy(wg.at[1, pl.ds(0, pw)], w1.at[d, pl.ds(k * pw, pw)], wr.at[d, k]).wait()
        product = 0.0
        for e in range(n):
            normed = nbuf[g, :, :, e * depth : (e + 1) * depth].reshape(chunk, depth)
            product = product + lax.dot_general(normed, w1[e], OVER_LAST, preferred_element_type=F32)
        parts = squares[g, 0]
        for d in range(1, n):
            parts = parts + squares[g, d]
        total = jnp.sum(parts.reshape(chunk, 128), axis=1, keepdims=True)
        own4[g, :, :, :edge] = product[:, :edge].reshape(n, share, edge)
        own4[g, :, :, edge:] = (product[:, edge:] + in_tile(total, 0.0)).reshape(n, share, 128)
        send4[g, :, :, :edge] = product[:, :edge].astype(BF16).reshape(n, share, edge)
        send4[g, :, :, edge:] = (product[:, edge:] + two_parts(total)).astype(BF16).reshape(n, share, 128)
        third = {
            d: send(send4.at[g, lax.rem(q + d, n)], recv4.at[g, d - 1], s4.at[g, d - 1], r4.at[g, d - 1], q_peer(d))
            for d in far_first(n)
        }
        yield
        total = own4[g, q]
        for d in near_first(n):
            third[d].wait_recv()
            total = total + recv4[g, d - 1].astype(F32)
        both = total * lax.rsqrt(all_squares(total[:, edge:]) / features + EPSILON)
        hid1[g, p, q] = (silu(both[:, :pw]) * both[:, pw : 2 * pw]).astype(BF16)
        yield from gather(hid1.at[g], semaphores[1 + g], 1, nothing, nothing)
        if g == 0:
            wait_down(1)
        product = 0.0
        for e in range(n):
            product = product + jnp.dot(hid1[g, e].reshape(chunk, pw), down1[e], preferred_element_type=F32)
        copies = send_along_z(1, g, product)
        yield
        mine = out.at[1 - c, g, z]
        out[1 - c, g, z] = sum_along_z(1, g, copies, stream[g, 0, z])
        rest = {d: send(mine, mine, so.at[g, 0, d - 1], ro.at[g, 0, d - 1], z_peer(d)) for d in far_first(nz)}
        passed = [send(mine, mine, so.at[g, 1, nz - 1], ro.at[g, 1, nz - 1], other)]
        for d in near_first(nz):
            yield
            rest[d].wait_recv()
            at = out.at[1 - c, g, lax.rem(z + nz - d, nz)]
            passed.append(send(at, at, so.at[g, 1, d - 1], ro.at[g, 1, d - 1], other))
        yield
        for copy in passed:
            copy.wait_recv()

    chunks = [finish(g) for g in range(CHUNKS)]
    for steps in chunks:
        next(steps)
    deal_parts("z")
    while chunks:
        for steps in list(chunks):
            if next(steps, chunks) is chunks:
                chunks.remove(steps)
    for copy in pending:
        copy.wait_send()
    deal_parts(None, False)


def first_cut(width):
    return pl.cdiv(2 * width, 256) * 128


def silu(v):
    return v / (1.0 + jnp.exp(-v))


CHUNKS = 2
DEAL = ('q', 'p', 'z', 'z')


def solution(mesh):
    nz = mesh.shape["cb"] // 2
    n = 4 if mesh.shape["ra"] == 16 else 2
    torus = Mesh(mesh.devices.reshape(n, n, nz, 2), ("y", "x", "z", "c"))
    ra, cb = ("y", "x"), ("z", "c")

    def body(tokens, norm_gain, gate_weight, up_weight, down_weight):
        count, depth = tokens.shape
        width = gate_weight.shape[2]
        pw = width * 2 // n
        half = count // 2
        group, zrows = half // n, half // nz // CHUNKS
        share = group // CHUNKS
        wide = pl.cdiv(2 * pw + 64, 128) * 128
        dma = pltpu.SemaphoreType.DMA
        rows = group // n
        cols = 128 + 2 * width
        scratch = [
            pltpu.VMEM((count, depth), BF16),
            pltpu.VMEM((CHUNKS, n, nz, zrows, depth), BF16),
            pltpu.VMEM((n, LAYERS, depth), F32),
            pltpu.VMEM((2 * width, depth), BF16),
            pltpu.VMEM((2, width, depth), BF16),
            pltpu.VMEM((n, wide, depth), BF16),
            pltpu.VMEM((n, pw, depth), BF16),
            pltpu.VMEM((CHUNKS, nz, zrows, n * depth), BF16),
            pltpu.VMEM((CHUNKS, n, nz, zrows, 128), F32),
            pltpu.VMEM((n, group, cols), F32),
            pltpu.VMEM((2, n, group, cols), BF16),
            pltpu.VMEM((2, n, group, cols), BF16),
            pltpu.VMEM((rows, 2 * cols - 128), F32),
            *[pltpu.VMEM((n - 1, rows, 2 * cols - 128), BF16)] * 2,
            pltpu.VMEM((n, n, rows, 2 * width), BF16),
            pltpu.VMEM((CHUNKS, n, share, wide), F32),
            pltpu.VMEM((CHUNKS, n, share, wide), BF16),
            pltpu.VMEM((CHUNKS, n - 1, share, wide), BF16),
            pltpu.VMEM((CHUNKS, n, n, share, pw), BF16),
            pltpu.VMEM((LAYERS, CHUNKS, nz, zrows, depth), F32),
            *[pltpu.VMEM((LAYERS, CHUNKS, nz - 1, zrows, depth), BF16)] * 2,
            pltpu.VMEM((CHUNKS, zrows, depth), BF16),
            pltpu.VMEM((2, width, depth), BF16),
            dma((7 + n // 2,)),
            *[dma((n - 1,))] * 2,
            dma((2, n // 2, 2)),
            dma((n, 2)),
            *[dma((1 + n // 2,))] * 2,
            *[dma((2, 2, n))] * 2,
            *[dma((2, n - 1))] * 2,
            *[dma((CHUNKS, n - 1))] * 2,
            *[dma((1 + CHUNKS, n - 1))] * 2,
            *[dma((1 + CHUNKS, n, n - 1))] * 2,
            *[dma((LAYERS, CHUNKS, nz - 1))] * 2,
            *[dma((CHUNKS, nz, n))] * 2,
            *[dma((CHUNKS, 2, nz))] * 2,
        ]
        result = pl.pallas_call(
            functools.partial(kernel, n, nz, depth * n * n),
            out_shape=jax.ShapeDtypeStruct((2, CHUNKS, nz, zrows, depth), BF16),
            in_specs=[pl.BlockSpec(memory_space=pl.ANY)] * 5,
            out_specs=pl.BlockSpec(memory_space=pltpu.VMEM),
            scratch_shapes=scratch,
            compiler_params=pltpu.CompilerParams(
                collective_id=0, has_side_effects=True, vmem_limit_bytes=24 * 1024 * 1024
            ),
        )(*(pltpu.with_memory_space_constraint(a, pltpu.HBM) for a in (tokens, norm_gain, jnp.swapaxes(gate_weight, 1, 2), jnp.swapaxes(up_weight, 1, 2), down_weight)))
        return result.reshape(count, depth)

    in_specs = (P(None, ra), P(None, ra), P(None, ra, cb), P(None, ra, cb), P(None, cb, ra))
    return jax.shard_map(body, mesh=torus, in_specs=in_specs, out_specs=P(None, ra), check_vma=False)
```

```python
import functools

import jax
import jax.numpy as jnp
from jax import lax
from jax.experimental import pallas as pl
from jax.experimental.pallas import tpu as pltpu
from jax.sharding import Mesh
from jax.sharding import PartitionSpec as P

MESH = pl.DeviceIdType.MESH
LAYERS = 2
EPSILON = 1e-06
KEEP = 0.5
F32 = jnp.float32
BF16 = jnp.bfloat16
OVER_LAST = (((1,), (1,)), ((), ()))


def far_first(n):
    return sorted(range(1, n), key=lambda d: (-min(d, n - d), d))


def near_first(n):
    return far_first(n)[::-1]


def kernel(n, nz, features, tok, gain, wg, wu, wd, out, *scratch):
    (
        tokens, stream, gains, w0, down0, w1, down1, nbuf, squares, own1, send1, recv1, own2, send2, recv2, hid0,
        own4, send4, recv4, hid1, part, send3, recv3, fresh,
        staged, load_sem, gs, gr, ws, wr, ds, dr, s1, r1, s2, r2, s4, r4, sq, rq, sp, rp, sz, rz, ss, rs, so, ro,
    ) = scratch
    y, x, z, c = (lax.axis_index(a) for a in ("y", "x", "z", "c"))
    _, _, _, zrows, depth = stream.shape
    chunk = nz * zrows
    half = CHUNKS * chunk
    group = half // n
    rows = group // n
    share = chunk // n
    width = wg.shape[1]
    pw = down1.shape[1]
    wide = w1.shape[1]
    halves = n // 2
    cut = first_cut(width)
    p = c * x + (1 - c) * y
    q = c * y + (1 - c) * x

    def p_peer(d):
        return {"y": lax.rem(y + (1 - c) * d, n), "x": lax.rem(x + c * d, n)}

    def q_peer(d):
        return {"y": lax.rem(y + c * d, n), "x": lax.rem(x + (1 - c) * d, n)}

    def z_peer(d):
        return {"z": lax.rem(z + d, nz)}

    other = {"c": 1 - c}
    pending = []

    def copy_to(src, dst, ss, rs, to):
        return pltpu.make_async_remote_copy(src, dst, ss, rs, device_id=to, device_id_type=MESH)

    def send(*where):
        copy = copy_to(*where)
        copy.start()
        pending.append(copy)
        return copy

    barrier = pltpu.get_barrier_semaphore()
    greeted = [p_peer(d) for d in range(1, n)] + [q_peer(d) for d in range(1, n)]
    greeted += [{**peer, "c": 1 - c} for peer in greeted]
    greeted += [z_peer(d) for d in range(1, nz)] + [{**z_peer(d), **other} for d in range(nz)]
    for peer in greeted:
        pl.semaphore_signal(barrier, 1, device_id=peer, device_id_type=MESH)

    loads = [
        pltpu.make_async_copy(gain, gains.at[0], load_sem.at[0]),
        pltpu.make_async_copy(tok, tokens, load_sem.at[1]),
        pltpu.make_async_copy(wg.at[0], w0.at[pl.ds(0, width)], load_sem.at[2]),
        pltpu.make_async_copy(wu.at[0], w0.at[pl.ds(width, width)], load_sem.at[3]),
    ]
    down_loads = [[pltpu.make_async_copy(wd.at[0], down0.at[0], load_sem.at[4])], [
        pltpu.make_async_copy(wd.at[1, pl.ds(h * pw, pw)], down1.at[c * halves + h], load_sem.at[5 + h])
        for h in range(halves)
    ]]
    part_loads = [
        pltpu.make_async_copy(w.at[1], staged.at[k], load_sem.at[5 + halves + k]) for k, w in enumerate((wg, wu))
    ]
    for copy in loads + down_loads[0] + down_loads[1] + part_loads:
        copy.start()
    w1[:, 2 * pw :, :] = jnp.zeros((n, wide - 2 * pw, depth), BF16)

    lane = lax.broadcasted_iota(jnp.int32, (1, 128), 1)
    edge = wide - 128

    def in_tile(high, low):
        return jnp.where(lane < 64, 0.0, jnp.where(lane < 96, high, low))

    def two_parts(total):
        high = total.astype(BF16).astype(F32)
        return in_tile(high, total - high)

    def all_squares(tile):
        return tile[:, 64:65] + tile[:, 96:97]

    for copy in loads:
        copy.wait()
    for at in range(2):
        mine = tokens[pl.ds((c if at == 0 else 1 - c) * half, half)].astype(F32)
        normed = (mine * gains[0, 0:1]).astype(BF16)
        product = lax.dot_general(normed, w0[...], OVER_LAST, preferred_element_type=F32)
        send1[at, :, :, 128:] = product.astype(BF16).reshape(n, group, 2 * width)
        if at == 0:
            own1[:, :, 128:] = product.reshape(n, group, 2 * width)
            total = jnp.sum(mine * mine, axis=1, keepdims=True)
            own1[:, :, :128] = in_tile(total, 0.0).reshape(n, group, 128)
            send1[0, :, :, :128] = two_parts(total).astype(BF16).reshape(n, group, 128)
    for copy in part_loads:
        copy.wait()
    pl.semaphore_wait(barrier, len(greeted))

    spans = [[pl.ds(0, 128 + cut), pl.ds(128 + cut, 2 * width - cut)], [pl.ds(128, cut), pl.ds(128 + cut, 2 * width - cut)]]
    first = {}
    for piece in range(2):
        for d in far_first(n) + [0]:
            for at in range(2):
                if at == 0 and d == 0:
                    continue
                to = lax.rem((p, q)[at] + d, n)
                first[piece, at, d] = send(
                    send1.at[at, to, :, spans[at][piece]],
                    recv1.at[at, d, :, spans[at][piece]],
                    s1.at[piece, at, d],
                    r1.at[piece, at, d],
                    {**(p_peer, q_peer)[at](d), "c": (c, 1 - c)[at]},
                )
    for d in far_first(n):
        send(gains.at[0], gains.at[d], gs.at[d - 1], gr.at[d - 1], p_peer(d))
    from_other = [[send(wd.at[0], down0.at[1], ds.at[0], dr.at[0], other)], [
        send(wd.at[1, pl.ds(h * pw, pw)], down1.at[c * halves + h], ds.at[1 + h], dr.at[1 + h], other)
        for h in range(halves)
    ]]

    def deal_parts(point, start=True):
        for t in range(2):
            a = x if t else y
            for h in range(halves):
                owner = c * halves + h
                d = lax.rem(owner - a + n, n)
                to = {"x" if t else "y": owner, "c": t}
                here = jnp.logical_and(c == t, owner == a)
                for k in range(2):
                    if start and DEAL[2 * k + h % 2] != point:
                        continue
                    src = staged.at[k, pl.ds(h * pw, pw)]
                    dst = w1.at[d, pl.ds(k * pw, pw)]
                    sem = ws.at[t, h, k]

                    @pl.when(jnp.logical_and(here, start))
                    def _():
                        pltpu.make_async_copy((wg, wu)[k].at[1, pl.ds(h * pw, pw)], dst, wr.at[d, k]).start()

                    @pl.when(jnp.logical_not(here))
                    def _():
                        copy = copy_to(src, dst, sem, wr.at[d, k], to)
                        if start:
                            copy.start()
                        else:
                            copy.wait_send()

    second = {}
    bounds = [0, 128 + 2 * cut, 128 + 4 * width]
    for piece in range(2):
        for d in near_first(n) + [0]:
            for at in range(2):
                if at == 1 or d:
                    first[piece, at, d].wait_recv()
        for d in far_first(n) + [0]:
            at = pl.ds(pl.multiple_of(lax.rem(q + d, n) * rows, rows), rows)
            mine = own1[p, at, spans[0][piece]]
            for e in range(1, n):
                mine = mine + recv1[0, e, at, spans[0][piece]].astype(F32)
            theirs = recv1[1, 0, at, spans[1][piece]].astype(F32)
            for e in range(1, n):
                theirs = theirs + recv1[1, e, at, spans[1][piece]].astype(F32)
            total = [mine, theirs]
            if piece == 0:
                norm = all_squares(mine[:, :128])
                tile = two_parts(norm) if d else in_tile(norm, 0.0)
                total = [tile, mine[:, 128:], theirs]
            total = jnp.concatenate(total, axis=1)
            span = pl.ds(bounds[piece], bounds[piece + 1] - bounds[piece])
            if d == 0:
                own2[:, span] = total
            else:
                send2[d - 1, :, span] = total.astype(BF16)
                second[piece, d] = send(
                    send2.at[d - 1, :, span], recv2.at[d - 1, :, span],
                    s2.at[piece, d - 1], r2.at[piece, d - 1], q_peer(d),
                )
    deal_parts("r")
    sums = []
    for piece in range(2):
        span = pl.ds(bounds[piece], bounds[piece + 1] - bounds[piece])
        total = own2[:, span]
        for d in near_first(n):
            second[piece, d].wait_recv()
            total = total + recv2[d - 1, :, span].astype(F32)
        sums.append(total)
    scale = lax.rsqrt(all_squares(sums[0][:, :128]) / features + EPSILON)
    rest = 2 * width - cut
    shares = []
    for at in range(2):
        both = [sums[0][:, 128 + at * cut : 128 + (at + 1) * cut], sums[1][:, at * rest : (at + 1) * rest]]
        both = jnp.concatenate(both, axis=1) * scale
        shares.append(silu(both[:, :width]) * both[:, width:])
    hid0[p, q] = jnp.concatenate(shares, axis=1).astype(BF16)

    def gather(hid, semaphores, layer, between, after):
        sq, rq, sp, rp = semaphores
        pieces = {}

        def spread(e):
            at = hid.at[p, lax.rem(q + n - e, n)]
            for d in far_first(n):
                pieces[e, d] = send(at, at, sp.at[e, d - 1], rp.at[e, d - 1], p_peer(d))

        at = hid.at[p, q]
        across = {d: send(at, at, sq.at[d - 1], rq.at[d - 1], q_peer(d)) for d in far_first(n)}
        spread(0)
        between()
        yield
        for d in near_first(n):
            across[d].wait_recv()
            spread(d)
        after()
        yield
        for e in [0] + near_first(n):
            for d in near_first(n):
                pieces[e, d].wait_recv()

    def send_along_z(layer, k, product):
        part[layer, k] = product.reshape(nz, zrows, depth)
        copies = {}
        for d in far_first(nz):
            at = (layer, k, d - 1)
            send3[at] = part[layer, k, lax.rem(z + d, nz)].astype(BF16)
            copies[d] = send(send3.at[at], recv3.at[at], sz.at[at], rz.at[at], z_peer(d))
        return copies

    def sum_along_z(layer, k, copies, before):
        branch = KEEP * before.astype(F32) + part[layer, k, z]
        for d in near_first(nz):
            copies[d].wait_recv()
            branch = branch + recv3[layer, k, d - 1].astype(F32)
        return branch.astype(BF16)

    def nothing():
        return None

    def wait_down(layer):
        for copy in down_loads[layer]:
            copy.wait()
        for copy in from_other[layer]:
            copy.wait_recv()

    semaphores = [tuple(s.at[k] for s in (sq, rq, sp, rp)) for k in range(1 + CHUNKS)]
    for _ in gather(hid0, semaphores[0], 0, lambda: deal_parts("q"), lambda: deal_parts("p")):
        pass
    wait_down(0)

    def normalize(g, d, k):
        mine = stream[g, d, k].astype(F32)
        nbuf[g, k, :, d * depth : (d + 1) * depth] = (mine * gains[d, 1:2]).astype(BF16)
        mine = mine * mine
        parts = mine[:, :128]
        for b in range(1, depth // 128):
            parts = parts + mine[:, b * 128 : (b + 1) * 128]
        squares[g, d, k] = parts

    def finish(g):
        lines = n // CHUNKS
        units = hid0[g * lines : (g + 1) * lines].reshape(chunk, 2 * width)
        product = jnp.dot(units, down0[...].reshape(2 * width, depth), preferred_element_type=F32)
        copies = send_along_z(0, g, product)
        yield
        before = tokens[pl.ds(pl.multiple_of(c * half + g * chunk + z * zrows, zrows), zrows)]
        fresh[g] = sum_along_z(0, g, copies, before)
        along = {
            d: send(fresh.at[g], stream.at[g, 0, z], ss.at[g, d, 0], rs.at[g, d, 0], {**z_peer(d), **other})
            for d in [0] + near_first(nz)
        }
        arriving = {}
        yield
        for e in [0] + near_first(nz):
            along[e].wait_recv()
            k = lax.rem(z + nz - e, nz)
            for d in far_first(n):
                arriving[e, d] = send(stream.at[g, 0, k], stream.at[g, d, k], ss.at[g, e, d], rs.at[g, e, d], p_peer(d))
        for k in range(nz):
            normalize(g, 0, k)
        if g == 0:
            for d in far_first(n):
                copy_to(gains.at[0], gains.at[d], gs.at[d - 1], gr.at[d - 1], p_peer(d)).wait_recv()
        yield
        for e in [0] + near_first(nz):
            for d in near_first(n):
                arriving[e, d].wait_recv()
                normalize(g, d, lax.rem(z + nz - e, nz))
        if g == 0:
            for d in range(n):
                for k in range(2):
                    pltpu.make_async_copy(wg.at[1, pl.ds(0, pw)], w1.at[d, pl.ds(k * pw, pw)], wr.at[d, k]).wait()
        product = 0.0
        for e in range(n):
            normed = nbuf[g, :, :, e * depth : (e + 1) * depth].reshape(chunk, depth)
            product = product + lax.dot_general(normed, w1[e], OVER_LAST, preferred_element_type=F32)
        parts = squares[g, 0]
        for d in range(1, n):
            parts = parts + squares[g, d]
        total = jnp.sum(parts.reshape(chunk, 128), axis=1, keepdims=True)
        own4[g, :, :, :edge] = product[:, :edge].reshape(n, share, edge)
        own4[g, :, :, edge:] = (product[:, edge:] + in_tile(total, 0.0)).reshape(n, share, 128)
        send4[g, :, :, :edge] = product[:, :edge].astype(BF16).reshape(n, share, edge)
        send4[g, :, :, edge:] = (product[:, edge:] + two_parts(total)).astype(BF16).reshape(n, share, 128)
        third = {
            d: send(send4.at[g, lax.rem(q + d, n)], recv4.at[g, d - 1], s4.at[g, d - 1], r4.at[g, d - 1], q_peer(d))
            for d in far_first(n)
        }
        yield
        total = own4[g, q]
        for d in near_first(n):
            third[d].wait_recv()
            total = total + recv4[g, d - 1].astype(F32)
        both = total * lax.rsqrt(all_squares(total[:, edge:]) / features + EPSILON)
        hid1[g, p, q] = (silu(both[:, :pw]) * both[:, pw : 2 * pw]).astype(BF16)
        yield from gather(hid1.at[g], semaphores[1 + g], 1, nothing, nothing)
        if g == 0:
            wait_down(1)
        product = 0.0
        for e in range(n):
            product = product + jnp.dot(hid1[g, e].reshape(chunk, pw), down1[e], preferred_element_type=F32)
        copies = send_along_z(1, g, product)
        yield
        mine = out.at[1 - c, g, z]
        out[1 - c, g, z] = sum_along_z(1, g, copies, stream[g, 0, z])
        rest = {d: send(mine, mine, so.at[g, 0, d - 1], ro.at[g, 0, d - 1], z_peer(d)) for d in far_first(nz)}
        passed = [send(mine, mine, so.at[g, 1, nz - 1], ro.at[g, 1, nz - 1], other)]
        for d in near_first(nz):
            yield
            rest[d].wait_recv()
            at = out.at[1 - c, g, lax.rem(z + nz - d, nz)]
            passed.append(send(at, at, so.at[g, 1, d - 1], ro.at[g, 1, d - 1], other))
        yield
        for copy in passed:
            copy.wait_recv()

    chunks = [finish(g) for g in range(CHUNKS)]
    for steps in chunks:
        next(steps)
    deal_parts("z")
    while chunks:
        for steps in list(chunks):
            if next(steps, chunks) is chunks:
                chunks.remove(steps)
    for copy in pending:
        copy.wait_send()
    deal_parts(None, False)


def first_cut(width):
    return pl.cdiv(2 * width, 256) * 128


def silu(v):
    return v / (1.0 + jnp.exp(-v))


CHUNKS = 2
DEAL = ('q', 'p', 'z', 'z')


def solution(mesh):
    nz = mesh.shape["cb"] // 2
    n = 4 if mesh.shape["ra"] == 16 else 2
    torus = Mesh(mesh.devices.reshape(n, n, nz, 2), ("y", "x", "z", "c"))
    ra, cb = ("y", "x"), ("z", "c")

    def body(tokens, norm_gain, gate_weight, up_weight, down_weight):
        count, depth = tokens.shape
        width = gate_weight.shape[2]
        pw = width * 2 // n
        half = count // 2
        group, zrows = half // n, half // nz // CHUNKS
        share = group // CHUNKS
        wide = pl.cdiv(2 * pw + 64, 128) * 128
        dma = pltpu.SemaphoreType.DMA
        rows = group // n
        cols = 128 + 2 * width
        scratch = [
            pltpu.VMEM((count, depth), BF16),
            pltpu.VMEM((CHUNKS, n, nz, zrows, depth), BF16),
            pltpu.VMEM((n, LAYERS, depth), F32),
            pltpu.VMEM((2 * width, depth), BF16),
            pltpu.VMEM((2, width, depth), BF16),
            pltpu.VMEM((n, wide, depth), BF16),
            pltpu.VMEM((n, pw, depth), BF16),
            pltpu.VMEM((CHUNKS, nz, zrows, n * depth), BF16),
            pltpu.VMEM((CHUNKS, n, nz, zrows, 128), F32),
            pltpu.VMEM((n, group, cols), F32),
            pltpu.VMEM((2, n, group, cols), BF16),
            pltpu.VMEM((2, n, group, cols), BF16),
            pltpu.VMEM((rows, 2 * cols - 128), F32),
            *[pltpu.VMEM((n - 1, rows, 2 * cols - 128), BF16)] * 2,
            pltpu.VMEM((n, n, rows, 2 * width), BF16),
            pltpu.VMEM((CHUNKS, n, share, wide), F32),
            pltpu.VMEM((CHUNKS, n, share, wide), BF16),
            pltpu.VMEM((CHUNKS, n - 1, share, wide), BF16),
            pltpu.VMEM((CHUNKS, n, n, share, pw), BF16),
            pltpu.VMEM((LAYERS, CHUNKS, nz, zrows, depth), F32),
            *[pltpu.VMEM((LAYERS, CHUNKS, nz - 1, zrows, depth), BF16)] * 2,
            pltpu.VMEM((CHUNKS, zrows, depth), BF16),
            pltpu.VMEM((2, width, depth), BF16),
            dma((7 + n // 2,)),
            *[dma((n - 1,))] * 2,
            dma((2, n // 2, 2)),
            dma((n, 2)),
            *[dma((1 + n // 2,))] * 2,
            *[dma((2, 2, n))] * 2,
            *[dma((2, n - 1))] * 2,
            *[dma((CHUNKS, n - 1))] * 2,
            *[dma((1 + CHUNKS, n - 1))] * 2,
            *[dma((1 + CHUNKS, n, n - 1))] * 2,
            *[dma((LAYERS, CHUNKS, nz - 1))] * 2,
            *[dma((CHUNKS, nz, n))] * 2,
            *[dma((CHUNKS, 2, nz))] * 2,
        ]
        result = pl.pallas_call(
            functools.partial(kernel, n, nz, depth * n * n),
            out_shape=jax.ShapeDtypeStruct((2, CHUNKS, nz, zrows, depth), BF16),
            in_specs=[pl.BlockSpec(memory_space=pl.ANY)] * 5,
            out_specs=pl.BlockSpec(memory_space=pltpu.VMEM),
            scratch_shapes=scratch,
            compiler_params=pltpu.CompilerParams(
                collective_id=0, has_side_effects=True, vmem_limit_bytes=24 * 1024 * 1024
            ),
        )(*(pltpu.with_memory_space_constraint(a, pltpu.HBM) for a in (tokens, norm_gain, jnp.swapaxes(gate_weight, 1, 2), jnp.swapaxes(up_weight, 1, 2), down_weight)))
        return result.reshape(count, depth)

    in_specs = (P(None, ra), P(None, ra), P(None, ra, cb), P(None, ra, cb), P(None, cb, ra))
    return jax.shard_map(body, mesh=torus, in_specs=in_specs, out_specs=P(None, ra), check_vma=False)
```
